128 devices in a mesh: sp: 32 (over y, x, core), tp: 4 (over z).
Axes of the slice: x: 4, y: 4, z: 4, core: 2. Of those that a mesh axis runs over, the one named last changes fastest.
Arguments:
- block_input: bfloat16 [4096, 1024], P('sp'), may hold values from -6 to 6
- w_query: bfloat16 [1024, 1024], P(None, 'tp'), may hold values from -0.1875 to 0.1875
- w_forget_fwd: bfloat16 [1024, 1024], P(None, 'tp'), may hold values from -0.1875 to 0.1875
- w_forget_bwd: bfloat16 [1024, 1024], P(None, 'tp'), may hold values from -0.1875 to 0.1875
- w_value: bfloat16 [1024, 1024], P(None, 'tp'), may hold values from -0.1875 to 0.1875
- floor_rate: float32 [2, 1024], P(None, 'tp'), may hold values from 0.2 to 6
- gain: float32 [128], replicated, may hold values from 0.1 to 1.9
- cotangent: bfloat16 [4096, 1024], P('sp', 'tp'), may hold values from -6 to 6
Outputs:
- grad_input: bfloat16 [4096, 1024], P(('sp', 'tp'))
- grad_query_weight: float32 [1024, 1024], P('sp', 'tp')
- grad_floor: float32 [2, 1024], P(None, 'tp')
The draws below stay inside these ranges and needn't reach their ends.
All inputs are finite; a program needn't handle non-finite values.
Results may differ from the reference program's by a relative error of at most 0.0045.
Values sent between devices are 32-bit elements.
No kernel may reach another device: no remote copies, remote signals or barrier semaphores. Data moves between devices by JAX's collectives and lax.ppermute only.
A program may use at most 64 MiB of HBM per device.

```python
import math
import jax
import jax.numpy as jnp
from jax import lax

HEADS = 8
KDIM = 128
VDIM = 128
D = 1024
TOK_DEV = 128
TOKENS = 4096


def with_spikes(result, rng, source, target, parts, factor):
    owner, partner = [(jnp.arange(result.shape[position]) // (result.shape[position] // parts)).reshape([-1 if axis == position else 1 for axis in range(result.ndim)]) for position in (source, target)]
    chosen = jax.random.permutation(rng, parts)[partner]
    strong = (owner == chosen) | (owner == (partner + parts // 2) % parts)
    return jnp.where(strong, factor * result, result)


def steps_of(own_key, dims, cuts, smallest, high):
    level = 1.0
    for position, blocks in cuts:
        steps = jax.random.uniform(jax.random.fold_in(jax.random.fold_in(own_key, 6), position), (blocks,), jnp.float32, smallest / len(cuts), high / len(cuts))
        level = level * jnp.repeat(jnp.exp(steps), dims[position] // blocks).reshape((-1,) + (1,) * (len(dims) - 1 - position))
    return level


def noise(rng, dims, scale, bound, cuts=(), dtype=jnp.bfloat16):
    level = steps_of(rng, dims, cuts, -0.22, 0.18) if cuts else 1.0
    array = jax.random.normal(rng, dims, jnp.float32) * scale * level
    return jnp.minimum(jnp.maximum(array, -bound), bound).astype(dtype)


def heavy_noise(key, shape, width, limit, split, heavy, kind=jnp.bfloat16):
    entries = width * jax.random.normal(key, shape, jnp.float32)
    if split:
        entries = entries * steps_of(key, shape, split, -0.22, 0.18)
    return jnp.clip(with_spikes(entries, jax.random.fold_in(key, 3), *heavy), -limit, limit).astype(kind)


def setup_inputs(seed: int = 0) -> dict:
    streams_of = jax.random.split(jax.random.key(seed), 9)
    return {
        "block_input": heavy_noise(streams_of[0], (TOKENS, D), 1.0, 6.0, ((0, 32),), (0, 1, 32, 2.75)),
        "w_query": noise(streams_of[1], (D, HEADS * KDIM), D ** -0.5, 0.1875, ((1, 4),)),
        "w_forget_fwd": noise(streams_of[2], (D, HEADS * KDIM), D ** -0.5, 0.1875, ((1, 4),)),
        "w_forget_bwd": noise(streams_of[3], (D, HEADS * KDIM), D ** -0.5, 0.1875, ((1, 4),)),
        "w_value": noise(streams_of[4], (D, HEADS * VDIM), D ** -0.5, 0.1875, ((1, 4),)),
        "floor_rate": jnp.clip(jnp.exp(math.log(6.0) - 3.4011974 * jax.random.uniform(streams_of[5], (2, HEADS * KDIM), jnp.float32) ** steps_of(streams_of[5], (2, HEADS * KDIM), ((1, 4),), -0.2, 0.2)), 0.2, 6.0),
        "gain": jnp.clip(1.0 + 0.18 * jax.random.normal(streams_of[6], (VDIM,), jnp.float32), 0.1, 1.9),
        "cotangent": noise(streams_of[7], (TOKENS, HEADS * VDIM), 1.0, 6.0, ((0, 32), (1, 4))),
    }


FINEST_ROUNDING = lax.Precision.HIGHEST
NORM_EPS = 1e-06

def gate_maps(raw_gate, floor_rates, seq_total):
    step_rate = floor_rates / seq_total
    opening = -jnp.expm1(-step_rate)
    log_forget = jnp.logaddexp(-step_rate, jnp.log(opening) + jax.nn.log_sigmoid(raw_gate))
    return (opening * jax.nn.sigmoid(-raw_gate), log_forget)

def span_output(queries, key_gate, log_forget, payload_entries, arriving_signal):
    cumul = jnp.cumsum(log_forget, axis=0)
    faded_asking_vector = queries * jnp.exp(cumul)
    k_dec = key_gate * jnp.exp(-cumul)
    tok_count = queries.shape[0]
    scores = jnp.einsum('thk,shk->hts', faded_asking_vector, k_dec, precision=FINEST_ROUNDING)
    scores = scores * jnp.tril(jnp.ones((tok_count, tok_count), jnp.float32))
    inner_part = jnp.einsum('hts,shv->thv', scores, payload_entries, precision=FINEST_ROUNDING)
    external_portion = jnp.einsum('nea,eaw->new', faded_asking_vector, arriving_signal, precision=FINEST_ROUNDING)
    return inner_part + external_portion

def span_carry(key_gate, log_forget, payload_entries):
    cumul = jnp.cumsum(log_forget, axis=0)
    final_running_total = cumul[-1]
    scaled_by_factor = key_gate * jnp.exp(final_running_total[None] - cumul)
    return (jnp.exp(final_running_total), jnp.einsum('xzp,xzo->zpo', scaled_by_factor, payload_entries, precision=FINEST_ROUNDING))

def normed(mixed, gain):
    mean_square = lax.optimization_barrier(jnp.mean(mixed * mixed, axis=-1, keepdims=True))
    return mixed * lax.rsqrt(mean_square + NORM_EPS) * gain

def run_direction(queries, key_gate, log_forget, payload_entries):
    seq_total, head_count, key_dim = queries.shape
    val_dim = payload_entries.shape[2]
    block_count = seq_total // TOK_DEV

    def blocks(source):
        return source.reshape((block_count, TOK_DEV) + source.shape[1:])

    def advance(carried, inputs):
        q_blk, k_blk, f_blk, v_blk = inputs
        mixed = span_output(q_blk, k_blk, f_blk, v_blk, carried)
        keep_all, local_sum = span_carry(k_blk, f_blk, v_blk)
        return (keep_all[..., None] * carried + local_sum, mixed)
    zero_state = jnp.zeros((head_count, key_dim, val_dim), jnp.float32)
    _, mixed_all = lax.scan(advance, zero_state, (blocks(queries), blocks(key_gate), blocks(log_forget), blocks(payload_entries)))
    return mixed_all.reshape(seq_total, head_count, val_dim)

def reference(block_input, w_query, w_forget_fwd, w_forget_bwd, w_value, floor_rate, gain, cotangent):
    seq_total = block_input.shape[0]

    def project(weight, per_head):
        pre = jnp.dot(block_input, weight, preferred_element_type=jnp.float32).astype(jnp.bfloat16)
        return lax.optimization_barrier(pre).astype(jnp.float32).reshape(seq_total, HEADS, per_head)
    raw_query = project(w_query, KDIM)
    raw_value = project(w_value, VDIM)
    raw_fwd = project(w_forget_fwd, KDIM)
    raw_bwd = project(w_forget_bwd, KDIM)
    floor_rates = floor_rate.reshape(2, HEADS, KDIM)

    def mixer(query_in, value_in, gate_fwd, gate_bwd, rate_pair):
        scaled = query_in * KDIM ** (-0.5)
        key_fwd, logf_fwd = gate_maps(gate_fwd, rate_pair[0], float(seq_total))
        key_bwd, logf_bwd = gate_maps(gate_bwd, rate_pair[1], float(seq_total))
        out_fwd = run_direction(scaled, key_fwd, logf_fwd, value_in)
        out_bwd = run_direction(jnp.flip(scaled, 0), jnp.flip(key_bwd, 0), jnp.flip(logf_bwd, 0), jnp.flip(value_in, 0))
        return normed(out_fwd + jnp.flip(out_bwd, 0), gain)
    _, mixer_back = jax.vjp(mixer, raw_query, raw_value, raw_fwd, raw_bwd, floor_rates)
    d_query, d_value, d_fwd, d_bwd, d_rates = mixer_back(cotangent.astype(jnp.float32).reshape(seq_total, HEADS, VDIM))
    g_query = d_query.reshape(seq_total, HEADS * KDIM).astype(jnp.bfloat16)
    g_fwd = d_fwd.reshape(seq_total, HEADS * KDIM).astype(jnp.bfloat16)
    g_bwd = d_bwd.reshape(seq_total, HEADS * KDIM).astype(jnp.bfloat16)
    g_value = d_value.reshape(seq_total, HEADS * VDIM).astype(jnp.bfloat16)
    summed = jnp.dot(g_query, w_query.T, preferred_element_type=jnp.float32)
    summed = summed + jnp.dot(g_fwd, w_forget_fwd.T, preferred_element_type=jnp.float32)
    summed = summed + jnp.dot(g_bwd, w_forget_bwd.T, preferred_element_type=jnp.float32)
    summed = summed + jnp.dot(g_value, w_value.T, preferred_element_type=jnp.float32)
    norm_scale = seq_total ** (-0.5)
    grad_weight = jnp.dot(block_input.T, g_query, preferred_element_type=jnp.float32) * norm_scale
    grad_floor = d_rates.reshape(2, HEADS * KDIM) * norm_scale
    return (summed.astype(jnp.bfloat16), grad_weight, grad_floor)
```

```python
import jax
import jax.numpy as jnp
from jax import lax
from jax.experimental import pallas as pl
from jax.experimental.pallas import tpu as pltpu
from jax.sharding import Mesh
from jax.sharding import PartitionSpec as P

SP = ("sp_0", "sp_1", "sp_2")
SP_TP = ("sp_0", "sp_1", "sp_2", "tp")
N = 32
T = 128
K = 128
HEADS = 2
W = HEADS * K
D = 1024
TOKENS = 4096.0
Q_SCALE = K ** (-0.5)
OUT_SCALE = TOKENS ** (-0.5)
NORM_EPS = 1e-06
F32 = jnp.float32
BF16 = jnp.bfloat16
NN = ((1,), (0,))
NT = ((1,), (1,))
VMEM = pl.BlockSpec(memory_space=pltpu.VMEM)
SMEM = pl.BlockSpec(memory_space=pltpu.SMEM)


def dot(a, b, dims):
    return lax.dot_general(a, b, (dims, ((), ())), preferred_element_type=F32)


def split(a):
    high = a.astype(BF16)
    return high, (a - high.astype(F32)).astype(BF16)


def dot3(a, b, dims):
    (ah, al), (bh, bl) = split(a), split(b)
    return dot(ah, bh, dims) + (dot(ah, bl, dims) + dot(al, bh, dims))


def dot2(a, b, dims):
    bh, bl = split(b)
    return dot(a, bh, dims) + dot(a, bl, dims)


def dot2r(a, b, dims):
    ah, al = split(a)
    return dot(ah, b, dims) + dot(al, b, dims)


def lower_triangle():
    row = lax.broadcasted_iota(jnp.int32, (T, T), 0)
    col = lax.broadcasted_iota(jnp.int32, (T, T), 1)
    return row >= col, row <= col


def opening_of(rate):
    r = rate * (1.0 / TOKENS)
    return r * (1.0 - r * (1 / 2) * (1.0 - r * (1 / 3) * (1.0 - r * (1 / 4))))


def gates(raw, opening):
    x = raw.astype(F32)
    closed = 1.0 / (1.0 + jnp.exp(x))
    return closed, opening * closed


def log_forget_of(key):
    return -key * (1.0 + key * (1 / 2 + key * (1 / 3 + key * (1 / 4 + key * (1 / 5)))))


def project_kernel(x_ref, wq_ref, wf_ref, wb_ref, wv_ref, rate_ref, q_ref, f_ref, b_ref, v_ref, cf_ref, cb_ref, msg_ref):
    x = x_ref[...]
    low, up = lower_triangle()
    low, up = low.astype(BF16), up.astype(BF16)
    v = dot(x, wv_ref[...], NN).astype(BF16)
    v_ref[...] = v
    opening = opening_of(rate_ref[...])
    decayed = []
    for d, (w_ref, raw_ref, cum_ref, tri) in enumerate(((wf_ref, f_ref, cf_ref, low), (wb_ref, b_ref, cb_ref, up))):
        raw = dot(x, w_ref[...], NN).astype(BF16)
        raw_ref[...] = raw
        _, key = gates(raw, opening[d : d + 1])
        cum = dot2(tri, log_forget_of(key), NN)
        cum_ref[...] = cum
        last = cum[T - 1 : T] if d == 0 else cum[0:1]
        decayed.append((jnp.exp(last), key * jnp.exp(last - cum)))
    for h in range(HEADS):
        cols = slice(h * K, (h + 1) * K)
        v_t = v[:, cols].astype(F32).T.astype(BF16)
        group = slice(h * 16, (h + 1) * 16)
        msg_ref[group, 16:24, :] = jnp.zeros((16, 8, K), F32)
        for d, (all_keep, left) in enumerate(decayed):
            state = dot2(v_t, left[:, cols], NN)
            msg_ref[group, 8 * d : 8 * d + 8, :] = state.reshape(16, 8, K)
            msg_ref[group, 16 + d : 17 + d, :] = jnp.broadcast_to(all_keep[:, cols].reshape(1, 1, K), (16, 1, K))
    q_ref[...] = dot(x, wq_ref[...], NN).astype(BF16)


def scan_kernel(got_ref, out_ref):
    run = jnp.zeros((8, K), F32)
    for j in range(N):
        out_ref[j, 0:8, :] = run
        run = got_ref[j, 16:17, :] * run + got_ref[j, 0:8, :]
    run = jnp.zeros((8, K), F32)
    for j in reversed(range(N)):
        out_ref[j, 8:16, :] = run
        run = got_ref[j, 17:18, :] * run + got_ref[j, 8:16, :]


def mix_kernel(
    core_ref, x_ref, q_ref, f_ref, b_ref, v_ref, cf_ref, cb_ref, rate_ref, gain_ref, cot_ref, in_ref,
    msg_ref, own_ref, other_ref, gq_ref, dv_ref, dbf_ref, dbb_ref, af_ref, ab_ref,
):
    low, up = lower_triangle()
    opening = opening_of(rate_ref[...])
    gain = gain_ref[...]
    grad_q = []
    for h in range(HEADS):
        cols = slice(h * K, (h + 1) * K)
        group = slice(h * 16, (h + 1) * 16)
        q = q_ref[:, cols].astype(F32) * Q_SCALE
        v = v_ref[:, cols]
        v_t = v.astype(F32).T.astype(BF16)
        parts = []
        for d, (raw_ref, cum_ref, tri) in enumerate(((f_ref, cf_ref, low), (b_ref, cb_ref, up))):
            closed, key = gates(raw_ref[:, cols], opening[d : d + 1, cols])
            cum = cum_ref[:, cols]
            grow = jnp.exp(cum)
            fade = jnp.exp(-cum)
            last = cum[T - 1 : T] if d == 0 else cum[0:1]
            state = in_ref[group, 8 * d : 8 * d + 8, :].reshape(K, K)
            parts.append((closed, key, grow, fade, last, q * grow, key * fade, state, tri))
        scores = jnp.zeros((T, T), F32)
        mixed = jnp.zeros((T, K), F32)
        for closed, key, grow, fade, last, a, b, state, tri in parts:
            scores = scores + jnp.where(tri, dot3(a, b, NT), 0.0)
            mixed = mixed + dot3(a, state, NT)
        mixed = mixed + dot2r(scores, v, NN)
        inv = lax.rsqrt(jnp.mean(mixed * mixed, axis=-1, keepdims=True) + NORM_EPS)
        scaled = cot_ref[:, cols].astype(F32) * gain
        d_mixed = inv * scaled - mixed * (inv * inv * inv * jnp.mean(scaled * mixed, axis=-1, keepdims=True))
        d_mixed_t = d_mixed.T
        d_scores = dot2r(d_mixed, v, NT)
        dv_ref[:, cols] = dot3(scores.T, d_mixed, NN)
        dq = jnp.zeros((T, K), F32)
        msg_ref[group, 32:40, :] = jnp.zeros((16, 8, K), F32)
        for d, (closed, key, grow, fade, last, a, b, state, tri) in enumerate(parts):
            local = jnp.where(tri, d_scores, 0.0)
            da = dot3(local, b, NN) + dot3(d_mixed, state, NN)
            db = dot3(local.T, a, NN)
            dq = dq + da * grow
            ada = a * da
            (dbf_ref, dbb_ref)[d][:, cols] = db
            (af_ref, ab_ref)[d][:, cols] = ada
            seed = dot3(d_mixed_t, a, NN)
            msg_ref[group, 8 * d : 8 * d + 8, :] = seed.reshape(16, 8, K)
            share = closed / (1.0 - key)
            before = dot2(tri.astype(BF16), share, NN)
            total = before[T - 1 : T] if d == 0 else before[0:1]
            keep = jnp.exp(last)
            z = keep * fade * (closed - (total - before) * key)
            reach = dot2(v_t, z, NN) - (keep * total) * state
            msg_ref[group, 16 + 8 * d : 24 + 8 * d, :] = reach.reshape(16, 8, K)
            floor = jnp.sum(closed * (db * fade) - before * (ada - b * db), axis=0, keepdims=True)
            msg_ref[h * 16, 32 + d : 33 + d, :] = floor
        grad_q.append((dq * Q_SCALE).astype(BF16))
    gq = jnp.concatenate(grad_q, axis=1)
    gq_ref[...] = gq
    term = dot(x_ref[...].astype(F32).T.astype(BF16), gq, NN).reshape(N, 2, 16, W)
    first = core_ref[0] == 0
    own = jnp.where(first, term[:, 0], term[:, 1])
    other = jnp.where(first, term[:, 1], term[:, 0])
    for part, ref in ((own, own_ref), (other, other_ref)):
        for h in range(HEADS):
            ref[:, 16 * h : 16 * h + 16, :] = part[:, :, h * K : (h + 1) * K]


def scan_back_kernel(keep_ref, got_ref, own_ref, other_ref, out_ref):
    run = jnp.zeros((8, K), F32)
    reach = jnp.zeros((8, K), F32)
    floor = jnp.zeros((1, K), F32)
    for j in reversed(range(N)):
        out_ref[j, 0:8, :] = run
        reach = reach + run * got_ref[j, 16:24, :]
        floor = floor + got_ref[j, 32:33, :]
        run = keep_ref[j, 16:17, :] * run + got_ref[j, 0:8, :]
    floor_fwd = floor + jnp.sum(reach, axis=0, keepdims=True)
    run = jnp.zeros((8, K), F32)
    reach = jnp.zeros((8, K), F32)
    floor = jnp.zeros((1, K), F32)
    for j in range(N):
        out_ref[j, 8:16, :] = run
        reach = reach + run * got_ref[j, 24:32, :]
        floor = floor + got_ref[j, 33:34, :]
        run = keep_ref[j, 17:18, :] * run + got_ref[j, 8:16, :]
    floor_bwd = floor + jnp.sum(reach, axis=0, keepdims=True)
    out_ref[:, 16:48, :] = own_ref[...] + other_ref[...]
    tail = jnp.concatenate([floor_fwd, floor_bwd, jnp.zeros((6, K), F32)], axis=0)
    out_ref[:, 48:56, :] = jnp.broadcast_to(tail[None], (N, 8, K))


def finish_kernel(
    f_ref, b_ref, v_ref, cf_ref, cb_ref, rate_ref, in_ref, got_ref,
    gq_ref, dv_ref, dbf_ref, dbb_ref, af_ref, ab_ref, wq_ref, wf_ref, wb_ref, wv_ref,
    term_ref, weight_ref, floor_ref,
):
    low, up = lower_triangle()
    rate = rate_ref[...]
    opening = opening_of(rate)
    g_raw = ([], [])
    g_value = []
    floor_rows = ([], [])
    for h in range(HEADS):
        cols = slice(h * K, (h + 1) * K)
        group = slice(h * 16, (h + 1) * 16)
        v = v_ref[:, cols]
        dv = dv_ref[:, cols]
        for d, (raw_ref, cum_ref, db_ref, ada_ref, rev) in enumerate(
            ((f_ref, cf_ref, dbf_ref, af_ref, up), (b_ref, cb_ref, dbb_ref, ab_ref, low))
        ):
            closed, key = gates(raw_ref[:, cols], opening[d : d + 1, cols])
            opened = 1.0 / (1.0 + jnp.exp(-raw_ref[:, cols].astype(F32)))
            cum = cum_ref[:, cols]
            fade = jnp.exp(-cum)
            last = cum[T - 1 : T] if d == 0 else cum[0:1]
            keep = jnp.exp(last)
            state = in_ref[group, 8 * d : 8 * d + 8, :].reshape(K, K)
            flow = got_ref[group, 8 * d : 8 * d + 8, :].reshape(K, K)
            b = key * fade
            left = b * keep
            d_left = dot2(v, flow, NN)
            dv = dv + dot3(left, flow, NT)
            db = db_ref[:, cols] + keep * d_left
            dc = ada_ref[:, cols] - b * db
            total = jnp.sum(left * d_left, axis=0, keepdims=True) + keep * jnp.sum(state * flow, axis=0, keepdims=True)
            d_log = dot2(rev.astype(BF16), dc, NN) + total
            whole = db * fade - d_log / (1.0 - key)
            g_raw[d].append((-key * opened * whole).astype(BF16))
            floor_rows[d].append(jnp.sum(got_ref[group, 48 + d : 49 + d, :], axis=0))
        g_value.append(dv.astype(BF16))
    out = dot(gq_ref[...], wq_ref[...], NT)
    out = out + dot(jnp.concatenate(g_raw[0], axis=1), wf_ref[...], NT)
    out = out + dot(jnp.concatenate(g_raw[1], axis=1), wb_ref[...], NT)
    out = out + dot(jnp.concatenate(g_value, axis=1), wv_ref[...], NT)
    term_ref[...] = out
    for c in range(2):
        acc = got_ref[c, 16:48, :]
        for j in range(1, N // 2):
            acc = acc + got_ref[2 * j + c, 16:48, :]
        for h in range(HEADS):
            weight_ref[16 * c : 16 * c + 16, h * K : (h + 1) * K] = acc[16 * h : 16 * h + 16] * OUT_SCALE
    shift = jnp.exp(rate * (-1.0 / TOKENS)) * (OUT_SCALE / TOKENS)
    for d in range(2):
        floor_ref[d : d + 1, :] = jnp.concatenate(floor_rows[d], axis=1) * shift[d : d + 1]


def shape(*dims, dtype=F32):
    return jax.ShapeDtypeStruct(dims, dtype)


def call(kernel, out_shape, specs, name):
    many = isinstance(out_shape, (tuple, list))
    return pl.pallas_call(
        kernel,
        out_shape=out_shape,
        in_specs=specs,
        out_specs=[VMEM] * len(out_shape) if many else VMEM,
        name=name,
    )


def exchange(array, axes):
    return lax.all_to_all(array, axes, 0, 0, tiled=True)


def body(x, w_query, w_forget_fwd, w_forget_bwd, w_value, floor_rate, gain, cotangent):
    tok = shape(T, W)
    tok16 = shape(T, W, dtype=BF16)
    q, f, b, v, cf, cb, sums = call(
        project_kernel, (tok16, tok16, tok16, tok16, tok, tok, shape(N, 24, K)), [VMEM] * 6, "project"
    )(x, w_query, w_forget_fwd, w_forget_bwd, w_value, floor_rate)
    sums = exchange(sums, SP)
    inflow = exchange(call(scan_kernel, shape(N, 16, K), [VMEM], "scan")(sums), SP)
    core = lax.axis_index("sp_2").reshape(1).astype(jnp.int32)
    seeds, own, other, gq, dv, dbf, dbb, af, ab = call(
        mix_kernel,
        (shape(N, 40, K), shape(N, 32, K), shape(N, 32, K), tok16, tok, tok, tok, tok, tok),
        [SMEM] + [VMEM] * 11,
        "mix",
    )(core, x, q, f, b, v, cf, cb, floor_rate, gain.reshape(1, K), cotangent, inflow)
    other = lax.ppermute(other, "sp_2", [(0, 1), (1, 0)])
    seeds = exchange(seeds, SP)
    outflow = exchange(
        call(scan_back_kernel, shape(N, 56, K), [VMEM] * 4, "scan_back")(sums, seeds, own, other), SP
    )
    term, grad_weight, grad_floor = call(
        finish_kernel, (shape(T, D), shape(N, W), shape(2, W)), [VMEM] * 18, "finish"
    )(
        f, b, v, cf, cb, floor_rate, inflow, outflow, gq, dv, dbf, dbb, af, ab,
        w_query, w_forget_fwd, w_forget_bwd, w_value,
    )
    pieces = exchange(term, "tp").reshape(4, T // 4, D)
    grad_input = (pieces[0] + pieces[1] + pieces[2] + pieces[3]).astype(BF16)
    return grad_input, grad_weight, grad_floor


def solution(mesh):
    finer = Mesh(mesh.devices.reshape(4, 4, 2, mesh.shape["tp"]), ("sp_0", "sp_1", "sp_2", "tp"))
    return jax.shard_map(
        body,
        mesh=finer,
        in_specs=(
            P(SP, None),
            P(None, "tp"),
            P(None, "tp"),
            P(None, "tp"),
            P(None, "tp"),
            P(None, "tp"),
            P(),
            P(SP, "tp"),
        ),
        out_specs=(P(SP_TP, None), P(SP, "tp"), P(None, "tp")),
        check_vma=False,
    )
```

```python
import jax
import jax.numpy as jnp
from jax import lax
from jax.experimental import pallas as pl
from jax.experimental.pallas import tpu as pltpu
from jax.sharding import Mesh
from jax.sharding import PartitionSpec as P

SP = ("sp_0", "sp_1", "sp_2")
SP_TP = ("sp_0", "sp_1", "sp_2", "tp")
N = 32
T = 128
K = 128
HEADS = 2
W = HEADS * K
D = 1024
TOKENS = 4096.0
Q_SCALE = K ** (-0.5)
OUT_SCALE = TOKENS ** (-0.5)
NORM_EPS = 1e-06
F32 = jnp.float32
BF16 = jnp.bfloat16
NN = ((1,), (0,))
NT = ((1,), (1,))
VMEM = pl.BlockSpec(memory_space=pltpu.VMEM)
SMEM = pl.BlockSpec(memory_space=pltpu.SMEM)
VMEM_LIMIT = 16 << 20
MANY, FEW = 400_000_000, 10_000_000


def dot(a, b, dims):
    return lax.dot_general(a, b, (dims, ((), ())), preferred_element_type=F32)


def split(a):
    high = a.astype(BF16)
    return high, (a - high.astype(F32)).astype(BF16)


def dot3(a, b, dims):
    (ah, al), (bh, bl) = split(a), split(b)
    return dot(ah, bh, dims) + (dot(ah, bl, dims) + dot(al, bh, dims))


def dot2(a, b, dims):
    bh, bl = split(b)
    return dot(a, bh, dims) + dot(a, bl, dims)


def dot2r(a, b, dims):
    ah, al = split(a)
    return dot(ah, b, dims) + dot(al, b, dims)


def lower_triangle():
    row = lax.broadcasted_iota(jnp.int32, (T, T), 0)
    col = lax.broadcasted_iota(jnp.int32, (T, T), 1)
    return row >= col, row <= col


def opening_of(rate):
    r = rate * (1.0 / TOKENS)
    return r * (1.0 - r * (1 / 2) * (1.0 - r * (1 / 3) * (1.0 - r * (1 / 4))))


def gates(raw, opening):
    x = raw.astype(F32)
    closed = 1.0 / (1.0 + jnp.exp(x))
    return closed, opening * closed


def log_forget_of(key):
    return -key * (1.0 + key * (1 / 2 + key * (1 / 3 + key * (1 / 4 + key * (1 / 5)))))


def project_kernel(x_ref, wf_ref, wb_ref, wv_ref, rate_ref, f_ref, b_ref, v_ref, cf_ref, cb_ref, msg_ref):
    x = x_ref[...]
    low, up = lower_triangle()
    low, up = low.astype(BF16), up.astype(BF16)
    v = dot(x, wv_ref[...], NN).astype(BF16)
    v_ref[...] = v
    opening = opening_of(rate_ref[...])
    decayed = []
    for d, (w_ref, raw_ref, cum_ref, tri) in enumerate(((wf_ref, f_ref, cf_ref, low), (wb_ref, b_ref, cb_ref, up))):
        raw = dot(x, w_ref[...], NN).astype(BF16)
        raw_ref[...] = raw
        _, key = gates(raw, opening[d : d + 1])
        cum = dot2(tri, log_forget_of(key), NN)
        cum_ref[...] = cum
        last = cum[T - 1 : T] if d == 0 else cum[0:1]
        decayed.append((jnp.exp(last), key * jnp.exp(last - cum)))
    for h in range(HEADS):
        cols = slice(h * K, (h + 1) * K)
        v_t = v[:, cols].astype(F32).T.astype(BF16)
        group = slice(h * 16, (h + 1) * 16)
        msg_ref[group, 16:24, :] = jnp.zeros((16, 8, K), F32)
        both = dot2(v_t, jnp.concatenate([left[:, cols] for _, left in decayed], axis=1), NN)
        for d, (all_keep, left) in enumerate(decayed):
            msg_ref[group, 8 * d : 8 * d + 8, :] = both[:, d * K : (d + 1) * K].reshape(16, 8, K)
            msg_ref[group, 16 + d : 17 + d, :] = jnp.broadcast_to(all_keep[:, cols].reshape(1, 1, K), (16, 1, K))


def local_kernel(
    x_ref, wq_ref, f_ref, b_ref, v_ref, cf_ref, cb_ref, rate_ref,
    a_ref, bk_ref, scores_ref, inner_ref, reach_ref, tail_ref, share_ref,
):
    low, up = lower_triangle()
    opening = opening_of(rate_ref[...])
    query = dot(x_ref[...], wq_ref[...], NN).astype(BF16).astype(F32) * Q_SCALE
    for h in range(HEADS):
        cols = slice(h * K, (h + 1) * K)
        v = v_ref[:, cols]
        v_t = v.astype(F32).T.astype(BF16)
        scores = jnp.zeros((T, T), F32)
        zs = []
        for d, (raw_ref, cum_ref, tri) in enumerate(((f_ref, cf_ref, low), (b_ref, cb_ref, up))):
            closed, key = gates(raw_ref[:, cols], opening[d : d + 1, cols])
            cum = cum_ref[:, cols]
            fade = jnp.exp(-cum)
            last = cum[T - 1 : T] if d == 0 else cum[0:1]
            a = query[:, cols] * jnp.exp(cum)
            b = key * fade
            both = slice((2 * h + d) * K, (2 * h + d + 1) * K)
            a_ref[:, both] = a
            bk_ref[:, both] = b
            scores = scores + jnp.where(tri, dot3(a, b, NT), 0.0)
            share = closed / (1.0 - key)
            before = dot2(tri.astype(BF16), share, NN)
            share_ref[:, both] = before
            total = before[T - 1 : T] if d == 0 else before[0:1]
            keep = jnp.exp(last)
            zs.append(keep * fade * (closed - (total - before) * key))
            tail_ref[2 * h + d : 2 * h + d + 1, :] = keep * total
        scores_ref[:, cols] = scores
        inner_ref[:, cols] = dot2r(scores, v, NN)
        reach_ref[:, 2 * h * K : 2 * (h + 1) * K] = dot2(v_t, jnp.concatenate(zs, axis=1), NN)


def scan_kernel(got_ref, out_ref):
    run_f = run_b = jnp.zeros((8, K), F32)
    for i in range(N):
        j = N - 1 - i
        out_ref[i, 0:8, :] = run_f
        out_ref[j, 8:16, :] = run_b
        run_f = got_ref[i, 16:17, :] * run_f + got_ref[i, 0:8, :]
        run_b = got_ref[j, 17:18, :] * run_b + got_ref[j, 8:16, :]


def states_of(ref, h):
    group = slice(h * 16, (h + 1) * 16)
    return [ref[group, 8 * d : 8 * d + 8, :].reshape(K, K) for d in range(2)]


def mix_kernel(a_ref, inner_ref, reach_ref, tail_ref, gain_ref, cot_ref, in_ref, msg_ref, dm_ref):
    gain = gain_ref[...]
    for h in range(HEADS):
        cols = slice(h * K, (h + 1) * K)
        wide = slice(2 * h * K, 2 * (h + 1) * K)
        group = slice(h * 16, (h + 1) * 16)
        a = a_ref[:, wide]
        states = jnp.concatenate(states_of(in_ref, h), axis=1)
        mixed = inner_ref[:, cols] + dot3(a, states, NT)
        inv = lax.rsqrt(jnp.mean(mixed * mixed, axis=-1, keepdims=True) + NORM_EPS)
        scaled = cot_ref[:, cols].astype(F32) * gain
        d_mixed = inv * scaled - mixed * (inv * inv * inv * jnp.mean(scaled * mixed, axis=-1, keepdims=True))
        dm_ref[:, cols] = d_mixed
        seeds = dot3(d_mixed.T, a, NN)
        tail = jnp.concatenate([tail_ref[2 * h + d : 2 * h + d + 1, :] for d in range(2)], axis=1)
        reach = reach_ref[:, wide] - tail * states
        for d in range(2):
            half = slice(d * K, (d + 1) * K)
            msg_ref[group, 8 * d : 8 * d + 8, :] = seeds[:, half].reshape(16, 8, K)
            msg_ref[group, 16 + 8 * d : 24 + 8 * d, :] = reach[:, half].reshape(16, 8, K)


def query_kernel(
    core_ref, x_ref, cf_ref, cb_ref, v_ref, a_ref, bk_ref, in_ref, dm_ref,
    own_ref, other_ref, gq_ref, local_ref, ada_ref,
):
    low, up = lower_triangle()
    grad_q = []
    for h in range(HEADS):
        cols = slice(h * K, (h + 1) * K)
        d_mixed = dm_ref[:, cols]
        d_scores = dot2r(d_mixed, v_ref[:, cols], NT)
        dq = jnp.zeros((T, K), F32)
        for d, (state, cum_ref, tri) in enumerate(zip(states_of(in_ref, h), (cf_ref, cb_ref), (low, up))):
            both = slice((2 * h + d) * K, (2 * h + d + 1) * K)
            local = jnp.where(tri, d_scores, 0.0)
            local_ref[:, both] = local
            da = dot3(
                jnp.concatenate([local, d_mixed], axis=1), jnp.concatenate([bk_ref[:, both], state], axis=0), NN
            )
            dq = dq + da * jnp.exp(cum_ref[:, cols])
            ada_ref[:, both] = a_ref[:, both] * da
        grad_q.append((dq * Q_SCALE).astype(BF16))
    gq = jnp.concatenate(grad_q, axis=1)
    gq_ref[...] = gq
    term = dot(x_ref[...].astype(F32).T.astype(BF16), gq, NN).reshape(N, 2, 16, W)
    first = core_ref[0] == 0
    own = jnp.where(first, term[:, 0], term[:, 1])
    other = jnp.where(first, term[:, 1], term[:, 0])
    for part, ref in ((own, own_ref), (other, other_ref)):
        for h in range(HEADS):
            ref[:, 16 * h : 16 * h + 16, :] = part[:, :, h * K : (h + 1) * K]


def key_kernel(
    f_ref, b_ref, cf_ref, cb_ref, rate_ref, a_ref, bk_ref, scores_ref, share_ref, local_ref, ada_ref, dm_ref,
    db_ref, dv_ref, floor_ref,
):
    opening = opening_of(rate_ref[...])
    for h in range(HEADS):
        cols = slice(h * K, (h + 1) * K)
        dv_ref[:, cols] = dot3(scores_ref[:, cols].T, dm_ref[:, cols], NN)
        for d, (raw_ref, cum_ref) in enumerate(((f_ref, cf_ref), (b_ref, cb_ref))):
            both = slice((2 * h + d) * K, (2 * h + d + 1) * K)
            db = dot3(local_ref[:, both].T, a_ref[:, both], NN)
            db_ref[:, both] = db
            closed, _ = gates(raw_ref[:, cols], opening[d : d + 1, cols])
            floor = closed * (db * jnp.exp(-cum_ref[:, cols])) - share_ref[:, both] * (
                ada_ref[:, both] - bk_ref[:, both] * db
            )
            floor_ref[2 * h + d : 2 * h + d + 1, :] = jnp.sum(floor, axis=0, keepdims=True)


def scan_back_kernel(keep_ref, got_ref, own_ref, other_ref, local_ref, out_ref):
    run_f = run_b = reach_f = reach_b = jnp.zeros((8, K), F32)
    for i in range(N):
        j = N - 1 - i
        out_ref[j, 0:8, :] = run_f
        out_ref[i, 8:16, :] = run_b
        reach_f = reach_f + run_f * got_ref[j, 16:24, :]
        reach_b = reach_b + run_b * got_ref[i, 24:32, :]
        run_f = keep_ref[j, 16:17, :] * run_f + got_ref[j, 0:8, :]
        run_b = keep_ref[i, 17:18, :] * run_b + got_ref[i, 8:16, :]
    out_ref[:, 16:48, :] = own_ref[...] + other_ref[...]
    tail = [jnp.sum(reach_f, axis=0, keepdims=True), jnp.sum(reach_b, axis=0, keepdims=True)]
    tail = jnp.concatenate(tail + [local_ref[...], jnp.zeros((2, K), F32)], axis=0)
    out_ref[:, 48:56, :] = jnp.broadcast_to(tail[None], (N, 8, K))


def first_term_kernel(gq_ref, wq_ref, term_ref):
    term_ref[...] = dot(gq_ref[...], wq_ref[...], NT)


def finish_kernel(
    f_ref, b_ref, v_ref, cf_ref, cb_ref, rate_ref, in_ref, got_ref,
    bk_ref, db_ref, dv_ref, ada_ref, first_ref, wf_ref, wb_ref, wv_ref,
    term_ref, weight_ref, floor_ref,
):
    low, up = lower_triangle()
    rate = rate_ref[...]
    opening = opening_of(rate)
    g_raw = ([], [])
    g_value = []
    rows = got_ref[:, 48:56, :]
    local_floor = jnp.sum(rows, axis=0)
    floors = ([], [])
    for h in range(HEADS):
        cols = slice(h * K, (h + 1) * K)
        wide = slice(2 * h * K, 2 * (h + 1) * K)
        flows = states_of(got_ref, h)
        flow = jnp.concatenate(flows, axis=1)
        states = states_of(in_ref, h)
        d_lefts = dot2(v_ref[:, cols], flow, NN)
        owned = jnp.sum(rows[h * 16 : (h + 1) * 16], axis=0)
        lefts = []
        for d, (raw_ref, cum_ref, rev) in enumerate(((f_ref, cf_ref, up), (b_ref, cb_ref, low))):
            both = slice((2 * h + d) * K, (2 * h + d + 1) * K)
            closed, key = gates(raw_ref[:, cols], opening[d : d + 1, cols])
            opened = 1.0 / (1.0 + jnp.exp(-raw_ref[:, cols].astype(F32)))
            cum = cum_ref[:, cols]
            last = cum[T - 1 : T] if d == 0 else cum[0:1]
            keep = jnp.exp(last)
            b = bk_ref[:, both]
            left = b * keep
            lefts.append(left)
            d_left = d_lefts[:, d * K : (d + 1) * K]
            db = db_ref[:, both] + keep * d_left
            dc = ada_ref[:, both] - b * db
            total = jnp.sum(left * d_left, axis=0, keepdims=True)
            total = total + keep * jnp.sum(states[d] * flows[d], axis=0, keepdims=True)
            d_log = dot2(rev.astype(BF16), dc, NN) + total
            whole = db * jnp.exp(-cum) - d_log / (1.0 - key)
            g_raw[d].append((-key * opened * whole).astype(BF16))
            floors[d].append(owned[d : d + 1] + local_floor[2 + 2 * h + d : 3 + 2 * h + d])
        dv = dv_ref[:, cols] + dot3(jnp.concatenate(lefts, axis=1), flow, NT)
        g_value.append(dv.astype(BF16))
    out = first_ref[...] + dot(jnp.concatenate(g_raw[0], axis=1), wf_ref[...], NT)
    out = out + dot(jnp.concatenate(g_raw[1], axis=1), wb_ref[...], NT)
    out = out + dot(jnp.concatenate(g_value, axis=1), wv_ref[...], NT)
    term_ref[...] = out
    for c in range(2):
        acc = got_ref[c, 16:48, :]
        for j in range(1, N // 2):
            acc = acc + got_ref[2 * j + c, 16:48, :]
        for h in range(HEADS):
            weight_ref[16 * c : 16 * c + 16, h * K : (h + 1) * K] = acc[16 * h : 16 * h + 16] * OUT_SCALE
    shift = jnp.exp(rate * (-1.0 / TOKENS)) * (OUT_SCALE / TOKENS)
    for d in range(2):
        floor_ref[d : d + 1, :] = jnp.concatenate(floors[d], axis=1) * shift[d : d + 1]


def shape(*dims, dtype=F32):
    return jax.ShapeDtypeStruct(dims, dtype)


def call(kernel, out_shape, specs, name, flops):
    many = isinstance(out_shape, (tuple, list))
    return pl.pallas_call(
        kernel,
        out_shape=out_shape,
        in_specs=specs,
        out_specs=[VMEM] * len(out_shape) if many else VMEM,
        name=name,
        cost_estimate=pl.CostEstimate(flops=flops, bytes_accessed=1 << 20, transcendentals=0),
        compiler_params=pltpu.CompilerParams(vmem_limit_bytes=VMEM_LIMIT),
    )


def exchange(array, axes):
    return lax.all_to_all(array, axes, 0, 0, tiled=True)


def body(x, w_query, w_forget_fwd, w_forget_bwd, w_value, floor_rate, gain, cotangent):
    tok, wide = shape(T, W), shape(T, 2 * W)
    tok16 = shape(T, W, dtype=BF16)
    f, b, v, cf, cb, sums = call(
        project_kernel, (tok16, tok16, tok16, tok, tok, shape(N, 24, K)), [VMEM] * 5, "project", MANY
    )(x, w_forget_fwd, w_forget_bwd, w_value, floor_rate)
    sums = exchange(sums, SP)
    a, bk, scores, inner, reach, tail, share = call(
        local_kernel, (wide, wide, tok, tok, wide, shape(4, K), wide), [VMEM] * 8, "local", MANY
    )(x, w_query, f, b, v, cf, cb, floor_rate)
    inflow = exchange(call(scan_kernel, shape(N, 16, K), [VMEM], "scan", FEW)(sums), SP)
    seeds, dm = call(mix_kernel, (shape(N, 32, K), tok), [VMEM] * 7, "mix", MANY)(
        a, inner, reach, tail, gain.reshape(1, K), cotangent, inflow
    )
    seeds = exchange(seeds, SP)
    core = lax.axis_index("sp_2").reshape(1).astype(jnp.int32)
    own, other, gq, local, ada = call(
        query_kernel, (shape(N, 32, K), shape(N, 32, K), tok16, wide, wide), [SMEM] + [VMEM] * 8, "query", MANY
    )(core, x, cf, cb, v, a, bk, inflow, dm)
    other = lax.ppermute(other, "sp_2", [(0, 1), (1, 0)])
    db, dv, floor = call(key_kernel, (wide, tok, shape(4, K)), [VMEM] * 12, "key", MANY)(
        f, b, cf, cb, floor_rate, a, bk, scores, share, local, ada, dm
    )
    outflow = exchange(
        call(scan_back_kernel, shape(N, 56, K), [VMEM] * 5, "scan_back", FEW)(sums, seeds, own, other, floor), SP
    )
    first = call(first_term_kernel, shape(T, D), [VMEM] * 2, "first_term", MANY)(gq, w_query)
    term, grad_weight, grad_floor = call(
        finish_kernel, (shape(T, D), shape(N, W), shape(2, W)), [VMEM] * 16, "finish", MANY
    )(
        f, b, v, cf, cb, floor_rate, inflow, outflow, bk, db, dv, ada, first, w_forget_fwd, w_forget_bwd, w_value
    )
    pieces = exchange(term, "tp").reshape(4, T // 4, D)
    grad_input = (pieces[0] + pieces[1] + pieces[2] + pieces[3]).astype(BF16)
    return grad_input, grad_weight, grad_floor


def solution(mesh):
    finer = Mesh(mesh.devices.reshape(4, 4, 2, mesh.shape["tp"]), ("sp_0", "sp_1", "sp_2", "tp"))
    return jax.shard_map(
        body,
        mesh=finer,
        in_specs=(
            P(SP, None),
            P(None, "tp"),
            P(None, "tp"),
            P(None, "tp"),
            P(None, "tp"),
            P(None, "tp"),
            P(),
            P(SP, "tp"),
        ),
        out_specs=(P(SP_TP, None), P(SP, "tp"), P(None, "tp")),
        check_vma=False,
    )
```

```python
import jax
import jax.numpy as jnp
from jax import lax
from jax.experimental import pallas as pl
from jax.experimental.pallas import tpu as pltpu
from jax.sharding import Mesh
from jax.sharding import PartitionSpec as P


SP = ("sp_0", "sp_1", "sp_2")
SP_TP = ("sp_0", "sp_1", "sp_2", "tp")
N = 32
T = 128
K = 128
HEADS = 2
W = HEADS * K
D = 1024
TOKENS = 4096.0
Q_SCALE = K ** (-0.5)
OUT_SCALE = TOKENS ** (-0.5)
NORM_EPS = 1e-06
F32 = jnp.float32
BF16 = jnp.bfloat16
NN = ((1,), (0,))
NT = ((1,), (1,))
VMEM = pl.BlockSpec(memory_space=pltpu.VMEM)
SMEM = pl.BlockSpec(memory_space=pltpu.SMEM)
HBM = pl.BlockSpec(memory_space=pltpu.HBM)
VMEM_LIMIT = 8 << 20
PROJECT_LIMIT = 67043328 - (900 << 10)
MANY, FEW = 400_000_000, 10_000_000


def dot(a, b, dims):
    return lax.dot_general(a, b, (dims, ((), ())), preferred_element_type=F32)


def split(a):
    high = a.astype(BF16)
    return high, (a - high.astype(F32)).astype(BF16)


def dot3(a, b, dims):
    (ah, al), (bh, bl) = split(a), split(b)
    return dot(ah, bh, dims) + (dot(ah, bl, dims) + dot(al, bh, dims))


def dot2(a, b, dims):
    bh, bl = split(b)
    return dot(a, bh, dims) + dot(a, bl, dims)


def dot2r(a, b, dims):
    ah, al = split(a)
    return dot(ah, b, dims) + dot(al, b, dims)


def lower_triangle():
    row = lax.broadcasted_iota(jnp.int32, (T, T), 0)
    col = lax.broadcasted_iota(jnp.int32, (T, T), 1)
    return row >= col, row <= col


def opening_of(rate):
    r = rate * (1.0 / TOKENS)
    return r * (1.0 - r * (1 / 2) * (1.0 - r * (1 / 3) * (1.0 - r * (1 / 4))))


def gates(raw, opening):
    x = raw.astype(F32)
    closed = 1.0 / (1.0 + jnp.exp(x))
    return closed, opening * closed


def log_forget_of(key):
    return -key * (1.0 + key * (1 / 2 + key * (1 / 3 + key * (1 / 4 + key * (1 / 5)))))


def fetch(sources, buffers, sems):
    def one(i):
        copy = pltpu.make_async_copy(sources[i], buffers[i], sems.at[i])
        copy.start()

        def value():
            copy.wait()
            return buffers[i][...]

        return value

    return [one(i) for i in range(len(sources))]


def project_kernel(
    x_hbm, wf_hbm, wb_hbm, wv_hbm, rate_hbm, f_ref, b_ref, v_ref, cf_ref, cb_ref, msg_ref, x_buf, w_buf, rate_buf, sems
):
    get_x, get_wf, get_rate, get_wb, get_wv = fetch(
        (x_hbm, wf_hbm, rate_hbm, wb_hbm, wv_hbm), (x_buf, w_buf.at[0], rate_buf, w_buf.at[1], w_buf.at[2]), sems
    )
    x = get_x()
    low, up = lower_triangle()
    low, up = low.astype(BF16), up.astype(BF16)
    opening = opening_of(get_rate())
    decayed = []
    for d, (get_w, raw_ref, cum_ref, tri) in enumerate(((get_wf, f_ref, cf_ref, low), (get_wb, b_ref, cb_ref, up))):
        raw = dot(x, get_w(), NN).astype(BF16)
        raw_ref[...] = raw
        _, key = gates(raw, opening[d : d + 1])
        cum = dot2(tri, log_forget_of(key), NN)
        cum_ref[...] = cum
        last = cum[T - 1 : T] if d == 0 else cum[0:1]
        decayed.append((jnp.exp(last), key * jnp.exp(last - cum)))
    v = dot(x, get_wv(), NN).astype(BF16)
    v_ref[...] = v
    for h in range(HEADS):
        cols = slice(h * K, (h + 1) * K)
        v_t = v[:, cols].astype(F32).T.astype(BF16)
        group = slice(h * 16, (h + 1) * 16)
        msg_ref[group, 16:24, :] = jnp.zeros((16, 8, K), F32)
        both = dot2(v_t, jnp.concatenate([left[:, cols] for _, left in decayed], axis=1), NN)
        for d, (all_keep, left) in enumerate(decayed):
            msg_ref[group, 8 * d : 8 * d + 8, :] = both[:, d * K : (d + 1) * K].reshape(16, 8, K)
            msg_ref[group, 16 + d : 17 + d, :] = jnp.broadcast_to(all_keep[:, cols].reshape(1, 1, K), (16, 1, K))


def local_kernel(
    x_hbm, wq_hbm, f_ref, b_ref, v_ref, cf_ref, cb_ref, rate_ref, gain_ref, cot_ref,
    a_ref, scores_ref, inner_ref, reach_ref, tail_ref, share_ref, scaled_ref, x_buf, w_buf, sems,
):
    get_x, get_wq = fetch((x_hbm, wq_hbm), (x_buf, w_buf), sems)
    low, up = lower_triangle()
    opening = opening_of(rate_ref[...])
    query = dot(get_x(), get_wq(), NN).astype(BF16).astype(F32) * Q_SCALE
    for h in range(HEADS):
        cols = slice(h * K, (h + 1) * K)
        v = v_ref[:, cols]
        v_t = v.astype(F32).T.astype(BF16)
        scores = jnp.zeros((T, T), F32)
        zs = []
        for d, (raw_ref, cum_ref, tri) in enumerate(((f_ref, cf_ref, low), (b_ref, cb_ref, up))):
            closed, key = gates(raw_ref[:, cols], opening[d : d + 1, cols])
            cum = cum_ref[:, cols]
            fade = jnp.exp(-cum)
            last = cum[T - 1 : T] if d == 0 else cum[0:1]
            a = query[:, cols] * jnp.exp(cum)
            b = key * fade
            both = slice((2 * h + d) * K, (2 * h + d + 1) * K)
            a_ref[:, both] = a
            scores = scores + jnp.where(tri, dot3(a, b, NT), 0.0)
            share = closed / (1.0 - key)
            before = dot2(tri.astype(BF16), share, NN)
            share_ref[:, both] = before
            total = before[T - 1 : T] if d == 0 else before[0:1]
            keep = jnp.exp(last)
            zs.append(keep * fade * (closed - (total - before) * key))
            tail_ref[2 * h + d : 2 * h + d + 1, :] = keep * total
        scores_ref[:, cols] = scores
        scaled_ref[:, cols] = cot_ref[:, cols].astype(F32) * gain_ref[...]
        inner_ref[:, cols] = dot2r(scores, v, NN)
        reach_ref[:, 2 * h * K : 2 * (h + 1) * K] = dot2(v_t, jnp.concatenate(zs, axis=1), NN)


def scan_kernel(got_ref, out_ref, keep_ref):
    keep_ref[...] = got_ref[:, 16:24, :]
    run_f = run_b = jnp.zeros((8, K), F32)
    for i in range(N):
        j = N - 1 - i
        out_ref[i, 0:8, :] = run_f
        out_ref[j, 8:16, :] = run_b
        run_f = got_ref[i, 16:17, :] * run_f + got_ref[i, 0:8, :]
        run_b = got_ref[j, 17:18, :] * run_b + got_ref[j, 8:16, :]


def states_of(ref, h):
    group = slice(h * 16, (h + 1) * 16)
    return [ref[group, 8 * d : 8 * d + 8, :].reshape(K, K) for d in range(2)]


def mix_kernel(a_ref, inner_ref, reach_ref, tail_ref, scaled_ref, in_ref, msg_ref, dm_ref):
    for h in range(HEADS):
        cols = slice(h * K, (h + 1) * K)
        wide = slice(2 * h * K, 2 * (h + 1) * K)
        group = slice(h * 16, (h + 1) * 16)
        a = a_ref[:, wide]
        states = jnp.concatenate(states_of(in_ref, h), axis=1)
        mixed = inner_ref[:, cols] + dot3(a, states, NT)
        inv = lax.rsqrt(jnp.mean(mixed * mixed, axis=-1, keepdims=True) + NORM_EPS)
        scaled = scaled_ref[:, cols]
        d_mixed = inv * scaled - mixed * (inv * inv * inv * jnp.mean(scaled * mixed, axis=-1, keepdims=True))
        dm_ref[:, cols] = d_mixed
        seeds = dot3(d_mixed.T, a, NN)
        tail = jnp.concatenate([tail_ref[2 * h + d : 2 * h + d + 1, :] for d in range(2)], axis=1)
        reach = reach_ref[:, wide] - tail * states
        for d in range(2):
            half = slice(d * K, (d + 1) * K)
            msg_ref[group, 8 * d : 8 * d + 8, :] = seeds[:, half].reshape(16, 8, K)
            msg_ref[group, 16 + 8 * d : 24 + 8 * d, :] = reach[:, half].reshape(16, 8, K)


def query_kernel(
    core_ref, x_hbm, f_ref, b_ref, cf_ref, cb_ref, rate_ref, v_ref, a_ref, in_ref, dm_ref,
    own_ref, other_ref, gq_ref, local_ref, ada_ref, x_buf, sems,
):
    (get_x,) = fetch((x_hbm,), (x_buf,), sems)
    low, up = lower_triangle()
    opening = opening_of(rate_ref[...])
    grad_q = []
    for h in range(HEADS):
        cols = slice(h * K, (h + 1) * K)
        d_mixed = dm_ref[:, cols]
        d_scores = dot2r(d_mixed, v_ref[:, cols], NT)
        dq = jnp.zeros((T, K), F32)
        for d, (state, raw_ref, cum_ref, tri) in enumerate(
            zip(states_of(in_ref, h), (f_ref, b_ref), (cf_ref, cb_ref), (low, up))
        ):
            _, key = gates(raw_ref[:, cols], opening[d : d + 1, cols])
            cum = cum_ref[:, cols]
            both = slice((2 * h + d) * K, (2 * h + d + 1) * K)
            local = jnp.where(tri, d_scores, 0.0)
            local_ref[:, both] = local
            da = dot3(
                jnp.concatenate([local, d_mixed], axis=1), jnp.concatenate([key * jnp.exp(-cum), state], axis=0), NN
            )
            dq = dq + da * jnp.exp(cum)
            ada_ref[:, both] = a_ref[:, both] * da
        grad_q.append((dq * Q_SCALE).astype(BF16))
    gq = jnp.concatenate(grad_q, axis=1)
    gq_ref[...] = gq
    term = dot(get_x().astype(F32).T.astype(BF16), gq, NN).reshape(N, 2, 16, W)
    first = core_ref[0] == 0
    own = jnp.where(first, term[:, 0], term[:, 1])
    other = jnp.where(first, term[:, 1], term[:, 0])
    for part, ref in ((own, own_ref), (other, other_ref)):
        for h in range(HEADS):
            ref[:, 16 * h : 16 * h + 16, :] = part[:, :, h * K : (h + 1) * K]


def key_kernel(
    f_ref, b_ref, cf_ref, cb_ref, rate_ref, a_ref, scores_ref, share_ref, local_ref, ada_ref, dm_ref,
    db_ref, dv_ref, floor_ref,
):
    opening = opening_of(rate_ref[...])
    for h in range(HEADS):
        cols = slice(h * K, (h + 1) * K)
        dv_ref[:, cols] = dot3(scores_ref[:, cols].T, dm_ref[:, cols], NN)
        for d, (raw_ref, cum_ref) in enumerate(((f_ref, cf_ref), (b_ref, cb_ref))):
            both = slice((2 * h + d) * K, (2 * h + d + 1) * K)
            db = dot3(local_ref[:, both].T, a_ref[:, both], NN)
            db_ref[:, both] = db
            closed, key = gates(raw_ref[:, cols], opening[d : d + 1, cols])
            faded = db * jnp.exp(-cum_ref[:, cols])
            floor = closed * faded - share_ref[:, both] * (ada_ref[:, both] - key * faded)
            floor_ref[2 * h + d : 2 * h + d + 1, :] = jnp.sum(floor, axis=0, keepdims=True)


def scan_back_kernel(keep_ref, got_ref, own_ref, other_ref, local_ref, out_ref):
    run_f = run_b = reach_f = reach_b = jnp.zeros((8, K), F32)
    for i in range(N):
        j = N - 1 - i
        out_ref[j, 0:8, :] = run_f
        out_ref[i, 8:16, :] = run_b
        reach_f = reach_f + run_f * got_ref[j, 16:24, :]
        reach_b = reach_b + run_b * got_ref[i, 24:32, :]
        run_f = keep_ref[j, 0:1, :] * run_f + got_ref[j, 0:8, :]
        run_b = keep_ref[i, 1:2, :] * run_b + got_ref[i, 8:16, :]
    out_ref[:, 16:48, :] = own_ref[...] + other_ref[...]
    tail = [jnp.sum(reach_f, axis=0, keepdims=True), jnp.sum(reach_b, axis=0, keepdims=True)]
    tail = jnp.concatenate(tail + [local_ref[...], jnp.zeros((2, K), F32)], axis=0)
    out_ref[:, 48:56, :] = jnp.broadcast_to(tail[None], (N, 8, K))


def finish_kernel(
    f_ref, b_ref, v_ref, cf_ref, cb_ref, rate_ref, in_ref, got_ref,
    db_ref, dv_ref, ada_ref, gq_ref, wq_hbm, wf_hbm, wb_hbm, wv_hbm,
    term_ref, weight_ref, floor_ref, w_buf, sems,
):
    weights = fetch((wq_hbm, wf_hbm, wb_hbm, wv_hbm), [w_buf.at[i] for i in range(4)], sems)
    low, up = lower_triangle()
    rate = rate_ref[...]
    opening = opening_of(rate)
    g_raw = ([], [])
    g_value = []
    rows = got_ref[:, 48:56, :]
    local_floor = jnp.sum(rows, axis=0)
    floors = ([], [])
    for h in range(HEADS):
        cols = slice(h * K, (h + 1) * K)
        flows = states_of(got_ref, h)
        flow = jnp.concatenate(flows, axis=1)
        states = states_of(in_ref, h)
        d_lefts = dot2(v_ref[:, cols], flow, NN)
        owned = jnp.sum(rows[h * 16 : (h + 1) * 16], axis=0)
        lefts = []
        for d, (raw_ref, cum_ref, rev) in enumerate(((f_ref, cf_ref, up), (b_ref, cb_ref, low))):
            both = slice((2 * h + d) * K, (2 * h + d + 1) * K)
            _, key = gates(raw_ref[:, cols], opening[d : d + 1, cols])
            opened = 1.0 / (1.0 + jnp.exp(-raw_ref[:, cols].astype(F32)))
            cum = cum_ref[:, cols]
            last = cum[T - 1 : T] if d == 0 else cum[0:1]
            keep = jnp.exp(last)
            fade = jnp.exp(-cum)
            b = key * fade
            left = b * keep
            lefts.append(left)
            d_left = d_lefts[:, d * K : (d + 1) * K]
            db = db_ref[:, both] + keep * d_left
            dc = ada_ref[:, both] - b * db
            total = jnp.sum(left * d_left, axis=0, keepdims=True)
            total = total + keep * jnp.sum(states[d] * flows[d], axis=0, keepdims=True)
            d_log = dot2(rev.astype(BF16), dc, NN) + total
            whole = db * fade - d_log / (1.0 - key)
            g_raw[d].append((-key * opened * whole).astype(BF16))
            floors[d].append(owned[d : d + 1] + local_floor[2 + 2 * h + d : 3 + 2 * h + d])
        dv = dv_ref[:, cols] + dot3(jnp.concatenate(lefts, axis=1), flow, NT)
        g_value.append(dv.astype(BF16))
    parts = [gq_ref[...]] + [jnp.concatenate(part, axis=1) for part in (g_raw[0], g_raw[1], g_value)]
    out = dot(parts[0], weights[0](), NT)
    for part, get_w in zip(parts[1:], weights[1:]):
        out = out + dot(part, get_w(), NT)
    term_ref[...] = out
    for c in range(2):
        acc = got_ref[c, 16:48, :]
        for j in range(1, N // 2):
            acc = acc + got_ref[2 * j + c, 16:48, :]
        for h in range(HEADS):
            weight_ref[16 * c : 16 * c + 16, h * K : (h + 1) * K] = acc[16 * h : 16 * h + 16] * OUT_SCALE
    shift = jnp.exp(rate * (-1.0 / TOKENS)) * (OUT_SCALE / TOKENS)
    for d in range(2):
        floor_ref[d : d + 1, :] = jnp.concatenate(floors[d], axis=1) * shift[d : d + 1]


def shape(*dims, dtype=F32):
    return jax.ShapeDtypeStruct(dims, dtype)


def call(kernel, out_shape, specs, flops, scratch=(), limit=VMEM_LIMIT):
    many = isinstance(out_shape, (tuple, list))
    return pl.pallas_call(
        kernel,
        out_shape=out_shape,
        in_specs=specs,
        out_specs=[VMEM] * len(out_shape) if many else VMEM,
        scratch_shapes=list(scratch),
        cost_estimate=pl.CostEstimate(flops=flops, bytes_accessed=1 << 20, transcendentals=0),
        compiler_params=pltpu.CompilerParams(vmem_limit_bytes=limit),
    )


def exchange(array, axes):
    return lax.all_to_all(array, axes, 0, 0, tiled=True)


def body(x, w_query, w_forget_fwd, w_forget_bwd, w_value, floor_rate, gain, cotangent):
    tok, wide = shape(T, W), shape(T, 2 * W)
    tok16 = shape(T, W, dtype=BF16)
    x_buf, w_buf = pltpu.VMEM((T, D), BF16), pltpu.VMEM((D, W), BF16)
    dma = pltpu.SemaphoreType.DMA
    f, b, v, cf, cb, sums = call(
        project_kernel, (tok16, tok16, tok16, tok, tok, shape(N, 24, K)), [HBM] * 5, MANY,
        (x_buf, pltpu.VMEM((3, D, W), BF16), pltpu.VMEM((2, W), F32), dma((5,))), PROJECT_LIMIT,
    )(x, w_forget_fwd, w_forget_bwd, w_value, floor_rate)
    sums = exchange(sums, SP)
    a, scores, inner, reach, tail, share, scaled = call(
        local_kernel, (wide, tok, tok, wide, shape(4, K), wide, tok), [HBM] * 2 + [VMEM] * 8, MANY,
        (x_buf, w_buf, dma((2,))),
    )(x, w_query, f, b, v, cf, cb, floor_rate, gain.reshape(1, K), cotangent)
    inflow, keeps = call(scan_kernel, (shape(N, 16, K), shape(N, 8, K)), [VMEM], FEW)(sums)
    inflow = exchange(inflow, SP)
    seeds, dm = call(mix_kernel, (shape(N, 32, K), tok), [VMEM] * 6, MANY)(
        a, inner, reach, tail, scaled, inflow
    )
    seeds = exchange(seeds, SP)
    core = lax.axis_index("sp_2").reshape(1).astype(jnp.int32)
    own, other, gq, local, ada = call(
        query_kernel, (shape(N, 32, K), shape(N, 32, K), tok16, wide, wide), [SMEM, HBM] + [VMEM] * 9,
        MANY, (x_buf, dma((1,))),
    )(core, x, f, b, cf, cb, floor_rate, v, a, inflow, dm)
    other = lax.ppermute(other, "sp_2", [(0, 1), (1, 0)])
    db, dv, floor = call(key_kernel, (wide, tok, shape(4, K)), [VMEM] * 11, MANY)(
        f, b, cf, cb, floor_rate, a, scores, share, local, ada, dm
    )
    outflow = exchange(call(scan_back_kernel, shape(N, 56, K), [VMEM] * 5, FEW)(keeps, seeds, own, other, floor), SP)
    term, grad_weight, grad_floor = call(
        finish_kernel, (shape(T, D), shape(N, W), shape(2, W)), [VMEM] * 12 + [HBM] * 4, MANY,
        (pltpu.VMEM((4, D, W), BF16), dma((4,))),
    )(
        f, b, v, cf, cb, floor_rate, inflow, outflow, db, dv, ada, gq,
        w_query, w_forget_fwd, w_forget_bwd, w_value,
    )
    pieces = exchange(term, "tp").reshape(4, T // 4, D)
    grad_input = (pieces[0] + pieces[1] + pieces[2] + pieces[3]).astype(BF16)
    return grad_input, grad_weight, grad_floor


def solution(mesh):
    finer = Mesh(mesh.devices.reshape(4, 4, 2, mesh.shape["tp"]), ("sp_0", "sp_1", "sp_2", "tp"))
    return jax.shard_map(
        body,
        mesh=finer,
        in_specs=(
            P(SP, None),
            P(None, "tp"),
            P(None, "tp"),
            P(None, "tp"),
            P(None, "tp"),
            P(None, "tp"),
            P(),
            P(SP, "tp"),
        ),
        out_specs=(P(SP_TP, None), P(SP, "tp"), P(None, "tp")),
        check_vma=False,
    )
```

```python
import jax
import jax.numpy as jnp
from jax import lax
from jax.experimental import pallas as pl
from jax.experimental.pallas import tpu as pltpu
from jax.sharding import Mesh
from jax.sharding import PartitionSpec as P


SP = ("sp_0", "sp_1", "sp_2")
SP_TP = ("sp_0", "sp_1", "sp_2", "tp")
N = 32
T = 128
K = 128
HEADS = 2
W = HEADS * K
D = 1024
TOKENS = 4096.0
Q_SCALE = K ** (-0.5)
OUT_SCALE = TOKENS ** (-0.5)
NORM_EPS = 1e-06
F32 = jnp.float32
BF16 = jnp.bfloat16
NN = ((1,), (0,))
NT = ((1,), (1,))
VMEM = pl.BlockSpec(memory_space=pltpu.VMEM)
SMEM = pl.BlockSpec(memory_space=pltpu.SMEM)
HBM = pl.BlockSpec(memory_space=pltpu.HBM)
VMEM_LIMIT = 8 << 20
PROJECT_LIMIT = 67043328 - (900 << 10)
MANY, FEW = 400_000_000, 10_000_000


def dot(a, b, dims):
    return lax.dot_general(a, b, (dims, ((), ())), preferred_element_type=F32)


def split(a):
    high = a.astype(BF16)
    return high, (a - high.astype(F32)).astype(BF16)


def dot3(a, b, dims):
    (ah, al), (bh, bl) = split(a), split(b)
    return dot(ah, bh, dims) + (dot(ah, bl, dims) + dot(al, bh, dims))


def dot2(a, b, dims):
    bh, bl = split(b)
    return dot(a, bh, dims) + dot(a, bl, dims)


def dot2r(a, b, dims):
    ah, al = split(a)
    return dot(ah, b, dims) + dot(al, b, dims)


def lower_triangle():
    row = lax.broadcasted_iota(jnp.int32, (T, T), 0)
    col = lax.broadcasted_iota(jnp.int32, (T, T), 1)
    return row >= col, row <= col


def opening_of(rate):
    r = rate * (1.0 / TOKENS)
    return r * (1.0 - r * (1 / 2) * (1.0 - r * (1 / 3) * (1.0 - r * (1 / 4))))


def gates(raw, opening):
    x = raw.astype(F32)
    closed = 1.0 / (1.0 + jnp.exp(x))
    return closed, opening * closed


def log_forget_of(key):
    return -key * (1.0 + key * (1 / 2 + key * (1 / 3 + key * (1 / 4 + key * (1 / 5)))))


def fetch(sources, buffers, sems):
    def one(i):
        copy = pltpu.make_async_copy(sources[i], buffers[i], sems.at[i])
        copy.start()

        def value():
            copy.wait()
            return buffers[i][...]

        return value

    return [one(i) for i in range(len(sources))]


def project_kernel(
    x_hbm, wf_hbm, wb_hbm, wv_hbm, rate_hbm, f_ref, b_ref, v_ref, msg_ref, x_buf, w_buf, rate_buf, sems
):
    get_x, get_wf, get_rate, get_wb, get_wv = fetch(
        (x_hbm, wf_hbm, rate_hbm, wb_hbm, wv_hbm), (x_buf, w_buf.at[0], rate_buf, w_buf.at[1], w_buf.at[2]), sems
    )
    x = get_x()
    low, up = lower_triangle()
    low, up = low.astype(BF16), up.astype(BF16)
    opening = opening_of(get_rate())
    decayed = []
    for d, (get_w, raw_ref, tri) in enumerate(((get_wf, f_ref, low), (get_wb, b_ref, up))):
        raw = dot(x, get_w(), NN).astype(BF16)
        raw_ref[...] = raw
        _, key = gates(raw, opening[d : d + 1])
        cum = dot2(tri, log_forget_of(key), NN)
        last = cum[T - 1 : T] if d == 0 else cum[0:1]
        decayed.append((jnp.exp(last), key * jnp.exp(last - cum)))
    v = dot(x, get_wv(), NN).astype(BF16)
    v_ref[...] = v
    for h in range(HEADS):
        cols = slice(h * K, (h + 1) * K)
        v_t = v[:, cols].astype(F32).T.astype(BF16)
        group = slice(h * 16, (h + 1) * 16)
        msg_ref[group, 16:24, :] = jnp.zeros((16, 8, K), F32)
        both = dot2(v_t, jnp.concatenate([left[:, cols] for _, left in decayed], axis=1), NN)
        for d, (all_keep, left) in enumerate(decayed):
            msg_ref[group, 8 * d : 8 * d + 8, :] = both[:, d * K : (d + 1) * K].reshape(16, 8, K)
            msg_ref[group, 16 + d : 17 + d, :] = jnp.broadcast_to(all_keep[:, cols].reshape(1, 1, K), (16, 1, K))


def local_kernel(
    x_hbm, wq_hbm, f_ref, b_ref, v_ref, rate_ref, gain_ref, cot_ref,
    cf_ref, cb_ref, a_ref, bk_ref, scores_ref, inner_ref, reach_ref, tail_ref, share_ref, scaled_ref, x_buf, w_buf, sems,
):
    get_x, get_wq = fetch((x_hbm, wq_hbm), (x_buf, w_buf), sems)
    low, up = lower_triangle()
    opening = opening_of(rate_ref[...])
    query = dot(get_x(), get_wq(), NN).astype(BF16).astype(F32) * Q_SCALE
    for h in range(HEADS):
        cols = slice(h * K, (h + 1) * K)
        v = v_ref[:, cols]
        v_t = v.astype(F32).T.astype(BF16)
        scores = jnp.zeros((T, T), F32)
        zs = []
        for d, (raw_ref, cum_ref, tri) in enumerate(((f_ref, cf_ref, low), (b_ref, cb_ref, up))):
            closed, key = gates(raw_ref[:, cols], opening[d : d + 1, cols])
            cum = dot2(tri.astype(BF16), log_forget_of(key), NN)
            cum_ref[:, cols] = cum
            fade = jnp.exp(-cum)
            last = cum[T - 1 : T] if d == 0 else cum[0:1]
            a = query[:, cols] * jnp.exp(cum)
            b = key * fade
            both = slice((2 * h + d) * K, (2 * h + d + 1) * K)
            a_ref[:, both] = a
            bk_ref[:, both] = b
            scores = scores + jnp.where(tri, dot3(a, b, NT), 0.0)
            share = closed / (1.0 - key)
            before = dot2(tri.astype(BF16), share, NN)
            share_ref[:, both] = before
            total = before[T - 1 : T] if d == 0 else before[0:1]
            keep = jnp.exp(last)
            zs.append(keep * fade * (closed - (total - before) * key))
            tail_ref[2 * h + d : 2 * h + d + 1, :] = keep * total
        scores_ref[:, cols] = scores
        scaled_ref[:, cols] = cot_ref[:, cols].astype(F32) * gain_ref[...]
        inner_ref[:, cols] = dot2r(scores, v, NN)
        reach_ref[:, 2 * h * K : 2 * (h + 1) * K] = dot2(v_t, jnp.concatenate(zs, axis=1), NN)


def scan_kernel(got_ref, out_ref):
    run_f = run_b = jnp.zeros((8, K), F32)
    for i in range(N):
        j = N - 1 - i
        out_ref[i, 0:8, :] = run_f
        out_ref[j, 8:16, :] = run_b
        run_f = got_ref[i, 16:17, :] * run_f + got_ref[i, 0:8, :]
        run_b = got_ref[j, 17:18, :] * run_b + got_ref[j, 8:16, :]


def states_of(ref, h):
    group = slice(h * 16, (h + 1) * 16)
    return [ref[group, 8 * d : 8 * d + 8, :].reshape(K, K) for d in range(2)]


def mix_kernel(a_ref, inner_ref, reach_ref, tail_ref, scaled_ref, in_ref, msg_ref, dm_ref):
    for h in range(HEADS):
        cols = slice(h * K, (h + 1) * K)
        wide = slice(2 * h * K, 2 * (h + 1) * K)
        group = slice(h * 16, (h + 1) * 16)
        a = a_ref[:, wide]
        states = jnp.concatenate(states_of(in_ref, h), axis=1)
        mixed = inner_ref[:, cols] + dot3(a, states, NT)
        inv = lax.rsqrt(jnp.mean(mixed * mixed, axis=-1, keepdims=True) + NORM_EPS)
        scaled = scaled_ref[:, cols]
        d_mixed = inv * scaled - mixed * (inv * inv * inv * jnp.mean(scaled * mixed, axis=-1, keepdims=True))
        dm_ref[:, cols] = d_mixed
        seeds = dot3(d_mixed.T, a, NN)
        tail = jnp.concatenate([tail_ref[2 * h + d : 2 * h + d + 1, :] for d in range(2)], axis=1)
        reach = reach_ref[:, wide] - tail * states
        for d in range(2):
            half = slice(d * K, (d + 1) * K)
            msg_ref[group, 8 * d : 8 * d + 8, :] = seeds[:, half].reshape(16, 8, K)
            msg_ref[group, 16 + 8 * d : 24 + 8 * d, :] = reach[:, half].reshape(16, 8, K)


def query_kernel(
    core_ref, x_hbm, cf_ref, cb_ref, v_ref, a_ref, bk_ref, in_ref, dm_ref,
    own_ref, other_ref, gq_ref, local_ref, ada_ref, x_buf, sems,
):
    (get_x,) = fetch((x_hbm,), (x_buf,), sems)
    low, up = lower_triangle()
    grad_q = []
    for h in range(HEADS):
        cols = slice(h * K, (h + 1) * K)
        d_mixed = dm_ref[:, cols]
        d_scores = dot2r(d_mixed, v_ref[:, cols], NT)
        dq = jnp.zeros((T, K), F32)
        for d, (state, cum_ref, tri) in enumerate(zip(states_of(in_ref, h), (cf_ref, cb_ref), (low, up))):
            both = slice((2 * h + d) * K, (2 * h + d + 1) * K)
            local = jnp.where(tri, d_scores, 0.0)
            local_ref[:, both] = local
            da = dot3(
                jnp.concatenate([local, d_mixed], axis=1), jnp.concatenate([bk_ref[:, both], state], axis=0), NN
            )
            dq = dq + da * jnp.exp(cum_ref[:, cols])
            ada_ref[:, both] = a_ref[:, both] * da
        grad_q.append((dq * Q_SCALE).astype(BF16))
    gq = jnp.concatenate(grad_q, axis=1)
    gq_ref[...] = gq
    term = dot(get_x().astype(F32).T.astype(BF16), gq, NN).reshape(N, 2, 16, W)
    first = core_ref[0] == 0
    own = jnp.where(first, term[:, 0], term[:, 1])
    other = jnp.where(first, term[:, 1], term[:, 0])
    for part, ref in ((own, own_ref), (other, other_ref)):
        for h in range(HEADS):
            ref[:, 16 * h : 16 * h + 16, :] = part[:, :, h * K : (h + 1) * K]


def key_kernel(
    f_ref, b_ref, cf_ref, cb_ref, rate_ref, a_ref, bk_ref, scores_ref, share_ref, local_ref, ada_ref, dm_ref,
    db_ref, dv_ref, floor_ref,
):
    opening = opening_of(rate_ref[...])
    for h in range(HEADS):
        cols = slice(h * K, (h + 1) * K)
        dv_ref[:, cols] = dot3(scores_ref[:, cols].T, dm_ref[:, cols], NN)
        for d, (raw_ref, cum_ref) in enumerate(((f_ref, cf_ref), (b_ref, cb_ref))):
            both = slice((2 * h + d) * K, (2 * h + d + 1) * K)
            db = dot3(local_ref[:, both].T, a_ref[:, both], NN)
            db_ref[:, both] = db
            closed, _ = gates(raw_ref[:, cols], opening[d : d + 1, cols])
            floor = closed * (db * jnp.exp(-cum_ref[:, cols])) - share_ref[:, both] * (
                ada_ref[:, both] - bk_ref[:, both] * db
            )
            floor_ref[2 * h + d : 2 * h + d + 1, :] = jnp.sum(floor, axis=0, keepdims=True)


def scan_back_kernel(keep_ref, got_ref, own_ref, other_ref, local_ref, out_ref):
    run_f = run_b = reach_f = reach_b = jnp.zeros((8, K), F32)
    for i in range(N):
        j = N - 1 - i
        out_ref[j, 0:8, :] = run_f
        out_ref[i, 8:16, :] = run_b
        reach_f = reach_f + run_f * got_ref[j, 16:24, :]
        reach_b = reach_b + run_b * got_ref[i, 24:32, :]
        run_f = keep_ref[j, 16:17, :] * run_f + got_ref[j, 0:8, :]
        run_b = keep_ref[i, 17:18, :] * run_b + got_ref[i, 8:16, :]
    out_ref[:, 16:48, :] = own_ref[...] + other_ref[...]
    tail = [jnp.sum(reach_f, axis=0, keepdims=True), jnp.sum(reach_b, axis=0, keepdims=True)]
    tail = jnp.concatenate(tail + [local_ref[...], jnp.zeros((2, K), F32)], axis=0)
    out_ref[:, 48:56, :] = jnp.broadcast_to(tail[None], (N, 8, K))


def finish_kernel(
    f_ref, b_ref, v_ref, cf_ref, cb_ref, rate_ref, in_ref, got_ref,
    db_ref, dv_ref, ada_ref, gq_ref, wq_hbm, wf_hbm, wb_hbm, wv_hbm,
    term_ref, weight_ref, floor_ref, w_buf, sems,
):
    weights = fetch((wq_hbm, wf_hbm, wb_hbm, wv_hbm), [w_buf.at[i] for i in range(4)], sems)
    low, up = lower_triangle()
    rate = rate_ref[...]
    opening = opening_of(rate)
    g_raw = ([], [])
    g_value = []
    rows = got_ref[:, 48:56, :]
    local_floor = jnp.sum(rows, axis=0)
    floors = ([], [])
    for h in range(HEADS):
        cols = slice(h * K, (h + 1) * K)
        flows = states_of(got_ref, h)
        flow = jnp.concatenate(flows, axis=1)
        states = states_of(in_ref, h)
        d_lefts = dot2(v_ref[:, cols], flow, NN)
        owned = jnp.sum(rows[h * 16 : (h + 1) * 16], axis=0)
        lefts = []
        for d, (raw_ref, cum_ref, rev) in enumerate(((f_ref, cf_ref, up), (b_ref, cb_ref, low))):
            both = slice((2 * h + d) * K, (2 * h + d + 1) * K)
            _, key = gates(raw_ref[:, cols], opening[d : d + 1, cols])
            opened = 1.0 / (1.0 + jnp.exp(-raw_ref[:, cols].astype(F32)))
            cum = cum_ref[:, cols]
            last = cum[T - 1 : T] if d == 0 else cum[0:1]
            keep = jnp.exp(last)
            fade = jnp.exp(-cum)
            b = key * fade
            left = b * keep
            lefts.append(left)
            d_left = d_lefts[:, d * K : (d + 1) * K]
            db = db_ref[:, both] + keep * d_left
            dc = ada_ref[:, both] - b * db
            total = jnp.sum(left * d_left, axis=0, keepdims=True)
            total = total + keep * jnp.sum(states[d] * flows[d], axis=0, keepdims=True)
            d_log = dot2(rev.astype(BF16), dc, NN) + total
            whole = db * fade - d_log / (1.0 - key)
            g_raw[d].append((-key * opened * whole).astype(BF16))
            floors[d].append(owned[d : d + 1] + local_floor[2 + 2 * h + d : 3 + 2 * h + d])
        dv = dv_ref[:, cols] + dot3(jnp.concatenate(lefts, axis=1), flow, NT)
        g_value.append(dv.astype(BF16))
    parts = [gq_ref[...]] + [jnp.concatenate(part, axis=1) for part in (g_raw[0], g_raw[1], g_value)]
    out = dot(parts[0], weights[0](), NT)
    for part, get_w in zip(parts[1:], weights[1:]):
        out = out + dot(part, get_w(), NT)
    term_ref[...] = out
    for c in range(2):
        acc = got_ref[c, 16:48, :]
        for j in range(1, N // 2):
            acc = acc + got_ref[2 * j + c, 16:48, :]
        for h in range(HEADS):
            weight_ref[16 * c : 16 * c + 16, h * K : (h + 1) * K] = acc[16 * h : 16 * h + 16] * OUT_SCALE
    shift = jnp.exp(rate * (-1.0 / TOKENS)) * (OUT_SCALE / TOKENS)
    for d in range(2):
        floor_ref[d : d + 1, :] = jnp.concatenate(floors[d], axis=1) * shift[d : d + 1]


def shape(*dims, dtype=F32):
    return jax.ShapeDtypeStruct(dims, dtype)


def call(kernel, out_shape, specs, flops, scratch=(), limit=VMEM_LIMIT):
    many = isinstance(out_shape, (tuple, list))
    return pl.pallas_call(
        kernel,
        out_shape=out_shape,
        in_specs=specs,
        out_specs=[VMEM] * len(out_shape) if many else VMEM,
        scratch_shapes=list(scratch),
        cost_estimate=pl.CostEstimate(flops=flops, bytes_accessed=1 << 20, transcendentals=0),
        compiler_params=pltpu.CompilerParams(vmem_limit_bytes=limit),
    )


def exchange(array, axes):
    return lax.all_to_all(array, axes, 0, 0, tiled=True)


def body(x, w_query, w_forget_fwd, w_forget_bwd, w_value, floor_rate, gain, cotangent):
    tok, wide = shape(T, W), shape(T, 2 * W)
    tok16 = shape(T, W, dtype=BF16)
    x_buf, w_buf = pltpu.VMEM((T, D), BF16), pltpu.VMEM((D, W), BF16)
    dma = pltpu.SemaphoreType.DMA
    f, b, v, sums = call(
        project_kernel, (tok16, tok16, tok16, shape(N, 24, K)), [HBM] * 5, MANY,
        (x_buf, pltpu.VMEM((3, D, W), BF16), pltpu.VMEM((2, W), F32), dma((5,))), PROJECT_LIMIT,
    )(x, w_forget_fwd, w_forget_bwd, w_value, floor_rate)
    sums = exchange(sums, SP)
    cf, cb, a, bk, scores, inner, reach, tail, share, scaled = call(
        local_kernel, (tok, tok, wide, wide, tok, tok, wide, shape(4, K), wide, tok), [HBM] * 2 + [VMEM] * 6, MANY,
        (x_buf, w_buf, dma((2,))),
    )(x, w_query, f, b, v, floor_rate, gain.reshape(1, K), cotangent)
    inflow = exchange(call(scan_kernel, shape(N, 16, K), [VMEM], FEW)(sums), SP)
    seeds, dm = call(mix_kernel, (shape(N, 32, K), tok), [VMEM] * 6, MANY)(
        a, inner, reach, tail, scaled, inflow
    )
    seeds = exchange(seeds, SP)
    core = lax.axis_index("sp_2").reshape(1).astype(jnp.int32)
    own, other, gq, local, ada = call(
        query_kernel, (shape(N, 32, K), shape(N, 32, K), tok16, wide, wide), [SMEM, HBM] + [VMEM] * 7,
        MANY, (x_buf, dma((1,))),
    )(core, x, cf, cb, v, a, bk, inflow, dm)
    other = lax.ppermute(other, "sp_2", [(0, 1), (1, 0)])
    db, dv, floor = call(key_kernel, (wide, tok, shape(4, K)), [VMEM] * 12, MANY)(
        f, b, cf, cb, floor_rate, a, bk, scores, share, local, ada, dm
    )
    outflow = exchange(call(scan_back_kernel, shape(N, 56, K), [VMEM] * 5, FEW)(sums, seeds, own, other, floor), SP)
    term, grad_weight, grad_floor = call(
        finish_kernel, (shape(T, D), shape(N, W), shape(2, W)), [VMEM] * 12 + [HBM] * 4, MANY,
        (pltpu.VMEM((4, D, W), BF16), dma((4,))),
    )(
        f, b, v, cf, cb, floor_rate, inflow, outflow, db, dv, ada, gq,
        w_query, w_forget_fwd, w_forget_bwd, w_value,
    )
    pieces = exchange(term, "tp").reshape(4, T // 4, D)
    grad_input = (pieces[0] + pieces[1] + pieces[2] + pieces[3]).astype(BF16)
    return grad_input, grad_weight, grad_floor


def solution(mesh):
    finer = Mesh(mesh.devices.reshape(4, 4, 2, mesh.shape["tp"]), ("sp_0", "sp_1", "sp_2", "tp"))
    return jax.shard_map(
        body,
        mesh=finer,
        in_specs=(
            P(SP, None),
            P(None, "tp"),
            P(None, "tp"),
            P(None, "tp"),
            P(None, "tp"),
            P(None, "tp"),
            P(),
            P(SP, "tp"),
        ),
        out_specs=(P(SP_TP, None), P(SP, "tp"), P(None, "tp")),
        check_vma=False,
    )
```

```python
import jax
import jax.numpy as jnp
from jax import lax
from jax.experimental import pallas as pl
from jax.experimental.pallas import tpu as pltpu
from jax.sharding import Mesh
from jax.sharding import PartitionSpec as P


SP = ("sp_0", "sp_1", "sp_2")
SP_TP = ("sp_0", "sp_1", "sp_2", "tp")
N = 32
T = 128
K = 128
HEADS = 2
W = HEADS * K
D = 1024
TOKENS = 4096.0
Q_SCALE = K ** (-0.5)
OUT_SCALE = TOKENS ** (-0.5)
NORM_EPS = 1e-06
F32 = jnp.float32
BF16 = jnp.bfloat16
NN = ((1,), (0,))
NT = ((1,), (1,))
VMEM = pl.BlockSpec(memory_space=pltpu.VMEM)
SMEM = pl.BlockSpec(memory_space=pltpu.SMEM)
HBM = pl.BlockSpec(memory_space=pltpu.HBM)
VMEM_LIMIT = 5 << 20
PROJECT_LIMIT = 67043328 - (900 << 10)
MANY, FEW = 400_000_000, 10_000_000


def dot(a, b, dims):
    return lax.dot_general(a, b, (dims, ((), ())), preferred_element_type=F32)


def split(a):
    high = a.astype(BF16)
    return high, (a - high.astype(F32)).astype(BF16)


def dot3(a, b, dims):
    (ah, al), (bh, bl) = split(a), split(b)
    return dot(ah, bh, dims) + (dot(ah, bl, dims) + dot(al, bh, dims))


def dot2(a, b, dims):
    bh, bl = split(b)
    return dot(a, bh, dims) + dot(a, bl, dims)


def dot2r(a, b, dims):
    ah, al = split(a)
    return dot(ah, b, dims) + dot(al, b, dims)


def lower_triangle():
    row = lax.broadcasted_iota(jnp.int32, (T, T), 0)
    col = lax.broadcasted_iota(jnp.int32, (T, T), 1)
    return row >= col, row <= col


def opening_of(rate):
    r = rate * (1.0 / TOKENS)
    return r * (1.0 - r * (1 / 2) * (1.0 - r * (1 / 3) * (1.0 - r * (1 / 4))))


def gates(raw, opening):
    x = raw.astype(F32)
    closed = 1.0 / (1.0 + jnp.exp(x))
    return closed, opening * closed


def log_forget_of(key):
    return -key * (1.0 + key * (1 / 2 + key * (1 / 3 + key * (1 / 4 + key * (1 / 5)))))


def fetch(sources, buffers, sems):
    def one(i):
        copy = pltpu.make_async_copy(sources[i], buffers[i], sems.at[i])
        copy.start()

        def value():
            copy.wait()
            return buffers[i][...]

        return value

    return [one(i) for i in range(len(sources))]


def project_kernel(
    x_hbm, wf_hbm, wb_hbm, wv_hbm, rate_hbm, f_ref, b_ref, v_ref, cf_ref, cb_ref, msg_ref, x_buf, w_buf, rate_buf, sems
):
    get_x, get_wf, get_rate, get_wb, get_wv = fetch(
        (x_hbm, wf_hbm, rate_hbm, wb_hbm, wv_hbm), (x_buf, w_buf.at[0], rate_buf, w_buf.at[1], w_buf.at[2]), sems
    )
    x = get_x()
    low, up = lower_triangle()
    low, up = low.astype(BF16), up.astype(BF16)
    opening = opening_of(get_rate())
    decayed = []
    for d, (get_w, raw_ref, cum_ref, tri) in enumerate(((get_wf, f_ref, cf_ref, low), (get_wb, b_ref, cb_ref, up))):
        raw = dot(x, get_w(), NN).astype(BF16)
        raw_ref[...] = raw
        _, key = gates(raw, opening[d : d + 1])
        cum = dot2(tri, log_forget_of(key), NN)
        cum_ref[...] = cum
        last = cum[T - 1 : T] if d == 0 else cum[0:1]
        decayed.append((jnp.exp(last), key * jnp.exp(last - cum)))
    v = dot(x, get_wv(), NN).astype(BF16)
    v_ref[...] = v
    for h in range(HEADS):
        cols = slice(h * K, (h + 1) * K)
        v_t = v[:, cols].astype(F32).T.astype(BF16)
        group = slice(h * 16, (h + 1) * 16)
        msg_ref[group, 16:24, :] = jnp.zeros((16, 8, K), F32)
        both = dot2(v_t, jnp.concatenate([left[:, cols] for _, left in decayed], axis=1), NN)
        for d, (all_keep, left) in enumerate(decayed):
            msg_ref[group, 8 * d : 8 * d + 8, :] = both[:, d * K : (d + 1) * K].reshape(16, 8, K)
            msg_ref[group, 16 + d : 17 + d, :] = jnp.broadcast_to(all_keep[:, cols].reshape(1, 1, K), (16, 1, K))


def local_kernel(
    x_hbm, wq_hbm, f_ref, b_ref, v_ref, cf_ref, cb_ref, rate_ref, gain_ref, cot_ref,
    a_ref, bk_ref, scores_ref, inner_ref, reach_ref, tail_ref, share_ref, scaled_ref, x_buf, w_buf, sems,
):
    get_x, get_wq = fetch((x_hbm, wq_hbm), (x_buf, w_buf), sems)
    low, up = lower_triangle()
    opening = opening_of(rate_ref[...])
    query = dot(get_x(), get_wq(), NN).astype(BF16).astype(F32) * Q_SCALE
    for h in range(HEADS):
        cols = slice(h * K, (h + 1) * K)
        v = v_ref[:, cols]
        v_t = v.astype(F32).T.astype(BF16)
        scores = jnp.zeros((T, T), F32)
        zs = []
        for d, (raw_ref, cum_ref, tri) in enumerate(((f_ref, cf_ref, low), (b_ref, cb_ref, up))):
            closed, key = gates(raw_ref[:, cols], opening[d : d + 1, cols])
            cum = cum_ref[:, cols]
            fade = jnp.exp(-cum)
            last = cum[T - 1 : T] if d == 0 else cum[0:1]
            a = query[:, cols] * jnp.exp(cum)
            b = key * fade
            both = slice((2 * h + d) * K, (2 * h + d + 1) * K)
            a_ref[:, both] = a
            bk_ref[:, both] = b
            scores = scores + jnp.where(tri, dot3(a, b, NT), 0.0)
            share = closed / (1.0 - key)
            before = dot2(tri.astype(BF16), share, NN)
            share_ref[:, both] = before
            total = before[T - 1 : T] if d == 0 else before[0:1]
            keep = jnp.exp(last)
            zs.append(keep * fade * (closed - (total - before) * key))
            tail_ref[2 * h + d : 2 * h + d + 1, :] = keep * total
        scores_ref[:, cols] = scores
        scaled_ref[:, cols] = cot_ref[:, cols].astype(F32) * gain_ref[...]
        inner_ref[:, cols] = dot2r(scores, v, NN)
        reach_ref[:, 2 * h * K : 2 * (h + 1) * K] = dot2(v_t, jnp.concatenate(zs, axis=1), NN)


def scan_kernel(got_ref, out_ref):
    run_f = run_b = jnp.zeros((8, K), F32)
    for i in range(N):
        j = N - 1 - i
        out_ref[i, 0:8, :] = run_f
        out_ref[j, 8:16, :] = run_b
        run_f = got_ref[i, 16:17, :] * run_f + got_ref[i, 0:8, :]
        run_b = got_ref[j, 17:18, :] * run_b + got_ref[j, 8:16, :]


def states_of(ref, h):
    group = slice(h * 16, (h + 1) * 16)
    return [ref[group, 8 * d : 8 * d + 8, :].reshape(K, K) for d in range(2)]


def mix_kernel(a_ref, inner_ref, reach_ref, tail_ref, scaled_ref, in_ref, msg_ref, dm_ref):
    for h in range(HEADS):
        cols = slice(h * K, (h + 1) * K)
        wide = slice(2 * h * K, 2 * (h + 1) * K)
        group = slice(h * 16, (h + 1) * 16)
        a = a_ref[:, wide]
        states = jnp.concatenate(states_of(in_ref, h), axis=1)
        mixed = inner_ref[:, cols] + dot3(a, states, NT)
        inv = lax.rsqrt(jnp.mean(mixed * mixed, axis=-1, keepdims=True) + NORM_EPS)
        scaled = scaled_ref[:, cols]
        d_mixed = inv * scaled - mixed * (inv * inv * inv * jnp.mean(scaled * mixed, axis=-1, keepdims=True))
        dm_ref[:, cols] = d_mixed
        seeds = dot3(d_mixed.T, a, NN)
        tail = jnp.concatenate([tail_ref[2 * h + d : 2 * h + d + 1, :] for d in range(2)], axis=1)
        reach = reach_ref[:, wide] - tail * states
        for d in range(2):
            half = slice(d * K, (d + 1) * K)
            msg_ref[group, 8 * d : 8 * d + 8, :] = seeds[:, half].reshape(16, 8, K)
            msg_ref[group, 16 + 8 * d : 24 + 8 * d, :] = reach[:, half].reshape(16, 8, K)


def query_kernel(
    core_ref, x_hbm, cf_ref, cb_ref, v_ref, a_ref, bk_ref, in_ref, dm_ref,
    own_ref, other_ref, gq_ref, local_ref, ada_ref, x_buf, sems,
):
    (get_x,) = fetch((x_hbm,), (x_buf,), sems)
    low, up = lower_triangle()
    grad_q = []
    for h in range(HEADS):
        cols = slice(h * K, (h + 1) * K)
        d_mixed = dm_ref[:, cols]
        d_scores = dot2r(d_mixed, v_ref[:, cols], NT)
        dq = jnp.zeros((T, K), F32)
        for d, (state, cum_ref, tri) in enumerate(zip(states_of(in_ref, h), (cf_ref, cb_ref), (low, up))):
            both = slice((2 * h + d) * K, (2 * h + d + 1) * K)
            local = jnp.where(tri, d_scores, 0.0)
            local_ref[:, both] = local
            da = dot3(
                jnp.concatenate([local, d_mixed], axis=1), jnp.concatenate([bk_ref[:, both], state], axis=0), NN
            )
            dq = dq + da * jnp.exp(cum_ref[:, cols])
            ada_ref[:, both] = a_ref[:, both] * da
        grad_q.append((dq * Q_SCALE).astype(BF16))
    gq = jnp.concatenate(grad_q, axis=1)
    gq_ref[...] = gq
    term = dot(get_x().astype(F32).T.astype(BF16), gq, NN).reshape(N, 2, 16, W)
    first = core_ref[0] == 0
    own = jnp.where(first, term[:, 0], term[:, 1])
    other = jnp.where(first, term[:, 1], term[:, 0])
    for part, ref in ((own, own_ref), (other, other_ref)):
        for h in range(HEADS):
            ref[:, 16 * h : 16 * h + 16, :] = part[:, :, h * K : (h + 1) * K]


def key_kernel(
    f_ref, b_ref, cf_ref, cb_ref, rate_ref, a_ref, bk_ref, scores_ref, share_ref, local_ref, ada_ref, dm_ref,
    db_ref, dv_ref, floor_ref,
):
    opening = opening_of(rate_ref[...])
    for h in range(HEADS):
        cols = slice(h * K, (h + 1) * K)
        dv_ref[:, cols] = dot3(scores_ref[:, cols].T, dm_ref[:, cols], NN)
        for d, (raw_ref, cum_ref) in enumerate(((f_ref, cf_ref), (b_ref, cb_ref))):
            both = slice((2 * h + d) * K, (2 * h + d + 1) * K)
            db = dot3(local_ref[:, both].T, a_ref[:, both], NN)
            db_ref[:, both] = db
            closed, _ = gates(raw_ref[:, cols], opening[d : d + 1, cols])
            floor = closed * (db * jnp.exp(-cum_ref[:, cols])) - share_ref[:, both] * (
                ada_ref[:, both] - bk_ref[:, both] * db
            )
            floor_ref[2 * h + d : 2 * h + d + 1, :] = jnp.sum(floor, axis=0, keepdims=True)


def scan_back_kernel(keep_ref, got_ref, own_ref, other_ref, local_ref, out_ref):
    run_f = run_b = reach_f = reach_b = jnp.zeros((8, K), F32)
    for i in range(N):
        j = N - 1 - i
        out_ref[j, 0:8, :] = run_f
        out_ref[i, 8:16, :] = run_b
        reach_f = reach_f + run_f * got_ref[j, 16:24, :]
        reach_b = reach_b + run_b * got_ref[i, 24:32, :]
        run_f = keep_ref[j, 16:17, :] * run_f + got_ref[j, 0:8, :]
        run_b = keep_ref[i, 17:18, :] * run_b + got_ref[i, 8:16, :]
    out_ref[:, 16:48, :] = own_ref[...] + other_ref[...]
    tail = [jnp.sum(reach_f, axis=0, keepdims=True), jnp.sum(reach_b, axis=0, keepdims=True)]
    tail = jnp.concatenate(tail + [local_ref[...], jnp.zeros((2, K), F32)], axis=0)
    out_ref[:, 48:56, :] = jnp.broadcast_to(tail[None], (N, 8, K))


def finish_kernel(
    f_ref, b_ref, v_ref, cf_ref, cb_ref, rate_ref, in_ref, got_ref,
    db_ref, dv_ref, ada_ref, gq_ref, wq_hbm, wf_hbm, wb_hbm, wv_hbm,
    term_ref, weight_ref, floor_ref, w_buf, sems,
):
    weights = fetch((wq_hbm, wf_hbm, wb_hbm, wv_hbm), [w_buf.at[i] for i in range(4)], sems)
    low, up = lower_triangle()
    rate = rate_ref[...]
    opening = opening_of(rate)
    g_raw = ([], [])
    g_value = []
    rows = got_ref[:, 48:56, :]
    local_floor = jnp.sum(rows, axis=0)
    floors = ([], [])
    for h in range(HEADS):
        cols = slice(h * K, (h + 1) * K)
        flows = states_of(got_ref, h)
        flow = jnp.concatenate(flows, axis=1)
        states = states_of(in_ref, h)
        d_lefts = dot2(v_ref[:, cols], flow, NN)
        owned = jnp.sum(rows[h * 16 : (h + 1) * 16], axis=0)
        lefts = []
        for d, (raw_ref, cum_ref, rev) in enumerate(((f_ref, cf_ref, up), (b_ref, cb_ref, low))):
            both = slice((2 * h + d) * K, (2 * h + d + 1) * K)
            _, key = gates(raw_ref[:, cols], opening[d : d + 1, cols])
            opened = 1.0 / (1.0 + jnp.exp(-raw_ref[:, cols].astype(F32)))
            cum = cum_ref[:, cols]
            last = cum[T - 1 : T] if d == 0 else cum[0:1]
            keep = jnp.exp(last)
            fade = jnp.exp(-cum)
            b = key * fade
            left = b * keep
            lefts.append(left)
            d_left = d_lefts[:, d * K : (d + 1) * K]
            db = db_ref[:, both] + keep * d_left
            dc = ada_ref[:, both] - b * db
            total = jnp.sum(left * d_left, axis=0, keepdims=True)
            total = total + keep * jnp.sum(states[d] * flows[d], axis=0, keepdims=True)
            d_log = dot2(rev.astype(BF16), dc, NN) + total
            whole = db * fade - d_log / (1.0 - key)
            g_raw[d].append((-key * opened * whole).astype(BF16))
            floors[d].append(owned[d : d + 1] + local_floor[2 + 2 * h + d : 3 + 2 * h + d])
        dv = dv_ref[:, cols] + dot3(jnp.concatenate(lefts, axis=1), flow, NT)
        g_value.append(dv.astype(BF16))
    parts = [gq_ref[...]] + [jnp.concatenate(part, axis=1) for part in (g_raw[0], g_raw[1], g_value)]
    out = dot(parts[0], weights[0](), NT)
    for part, get_w in zip(parts[1:], weights[1:]):
        out = out + dot(part, get_w(), NT)
    term_ref[...] = out
    for c in range(2):
        acc = got_ref[c, 16:48, :]
        for j in range(1, N // 2):
            acc = acc + got_ref[2 * j + c, 16:48, :]
        for h in range(HEADS):
            weight_ref[16 * c : 16 * c + 16, h * K : (h + 1) * K] = acc[16 * h : 16 * h + 16] * OUT_SCALE
    shift = jnp.exp(rate * (-1.0 / TOKENS)) * (OUT_SCALE / TOKENS)
    for d in range(2):
        floor_ref[d : d + 1, :] = jnp.concatenate(floors[d], axis=1) * shift[d : d + 1]


def shape(*dims, dtype=F32):
    return jax.ShapeDtypeStruct(dims, dtype)


def call(kernel, out_shape, specs, flops, scratch=(), limit=VMEM_LIMIT):
    many = isinstance(out_shape, (tuple, list))
    return pl.pallas_call(
        kernel,
        out_shape=out_shape,
        in_specs=specs,
        out_specs=[VMEM] * len(out_shape) if many else VMEM,
        scratch_shapes=list(scratch),
        cost_estimate=pl.CostEstimate(flops=flops, bytes_accessed=1 << 20, transcendentals=0),
        compiler_params=pltpu.CompilerParams(vmem_limit_bytes=limit),
    )


def exchange(array, axes):
    return lax.all_to_all(array, axes, 0, 0, tiled=True)


def body(x, w_query, w_forget_fwd, w_forget_bwd, w_value, floor_rate, gain, cotangent):
    tok, wide = shape(T, W), shape(T, 2 * W)
    tok16 = shape(T, W, dtype=BF16)
    x_buf, w_buf = pltpu.VMEM((T, D), BF16), pltpu.VMEM((D, W), BF16)
    dma = pltpu.SemaphoreType.DMA
    f, b, v, cf, cb, sums = call(
        project_kernel, (tok16, tok16, tok16, tok, tok, shape(N, 24, K)), [HBM] * 5, MANY,
        (x_buf, pltpu.VMEM((3, D, W), BF16), pltpu.VMEM((2, W), F32), dma((5,))), PROJECT_LIMIT,
    )(x, w_forget_fwd, w_forget_bwd, w_value, floor_rate)
    sums = exchange(sums, SP)
    a, bk, scores, inner, reach, tail, share, scaled = call(
        local_kernel, (wide, wide, tok, tok, wide, shape(4, K), wide, tok), [HBM] * 2 + [VMEM] * 8, MANY,
        (x_buf, w_buf, dma((2,))),
    )(x, w_query, f, b, v, cf, cb, floor_rate, gain.reshape(1, K), cotangent)
    inflow = exchange(call(scan_kernel, shape(N, 16, K), [VMEM], FEW)(sums), SP)
    seeds, dm = call(mix_kernel, (shape(N, 32, K), tok), [VMEM] * 6, MANY)(
        a, inner, reach, tail, scaled, inflow
    )
    seeds = exchange(seeds, SP)
    core = lax.axis_index("sp_2").reshape(1).astype(jnp.int32)
    own, other, gq, local, ada = call(
        query_kernel, (shape(N, 32, K), shape(N, 32, K), tok16, wide, wide), [SMEM, HBM] + [VMEM] * 7,
        MANY, (x_buf, dma((1,))),
    )(core, x, cf, cb, v, a, bk, inflow, dm)
    other = lax.ppermute(other, "sp_2", [(0, 1), (1, 0)])
    db, dv, floor = call(key_kernel, (wide, tok, shape(4, K)), [VMEM] * 12, MANY)(
        f, b, cf, cb, floor_rate, a, bk, scores, share, local, ada, dm
    )
    outflow = exchange(call(scan_back_kernel, shape(N, 56, K), [VMEM] * 5, FEW)(sums, seeds, own, other, floor), SP)
    term, grad_weight, grad_floor = call(
        finish_kernel, (shape(T, D), shape(N, W), shape(2, W)), [VMEM] * 12 + [HBM] * 4, MANY,
        (pltpu.VMEM((4, D, W), BF16), dma((4,))),
    )(
        f, b, v, cf, cb, floor_rate, inflow, outflow, db, dv, ada, gq,
        w_query, w_forget_fwd, w_forget_bwd, w_value,
    )
    pieces = exchange(term, "tp").reshape(4, T // 4, D)
    grad_input = (pieces[0] + pieces[1] + pieces[2] + pieces[3]).astype(BF16)
    return grad_input, grad_weight, grad_floor


def solution(mesh):
    finer = Mesh(mesh.devices.reshape(4, 4, 2, mesh.shape["tp"]), ("sp_0", "sp_1", "sp_2", "tp"))
    return jax.shard_map(
        body,
        mesh=finer,
        in_specs=(
            P(SP, None),
            P(None, "tp"),
            P(None, "tp"),
            P(None, "tp"),
            P(None, "tp"),
            P(None, "tp"),
            P(),
            P(SP, "tp"),
        ),
        out_specs=(P(SP_TP, None), P(SP, "tp"), P(None, "tp")),
        check_vma=False,
    )
```
